128 devices in a mesh: sp: 64 (over z, y, x), tp: 2 (over core).
Axes of the slice: x: 4, y: 4, z: 4, core: 2. Of those that a mesh axis runs over, the one named last changes fastest.
Arguments:
- residual: bfloat16 [16384, 2048], P(('sp', 'tp')), may hold values from -6 to 6
- queries: bfloat16 [16384, 1152], P('sp', 'tp'), may hold values from -800 to 800
- latent: bfloat16 [16384, 256], P('sp'), may hold values from -6 to 6
- rope_key: bfloat16 [16384, 32], P('sp'), may hold values from -6 to 6
- doc_ids: int32 [16384], P('sp'), may hold values from 0 to 5, never falling along the last dimension, each value on 1 to 8192 neighbouring positions
- latent_to_key: bfloat16 [256, 768], P(None, 'tp'), may hold values from -0.375 to 0.375
- latent_to_value: bfloat16 [256, 768], P(None, 'tp'), may hold values from -0.375 to 0.375
- out_proj: bfloat16 [768, 2048], replicated, may hold values from -0.21875 to 0.21875
- mix_gain: float32 [2048], replicated, may hold values from 0.1 to 1.9
- moe_gain: float32 [2048], replicated, may hold values from 0.1 to 1.9
- expert_ids: int32 [16384, 2], P(('sp', 'tp')), may hold values from 0 to 63, as said below
- route_weight: float32 [16384, 2], P(('sp', 'tp')), may hold values from 0.1 to 1
- gate_weight: bfloat16 [64, 2048, 1024], P('sp', None, 'tp'), may hold values from -0.125 to 0.125
- up_weight: bfloat16 [64, 2048, 1024], P('sp', None, 'tp'), may hold values from -0.125 to 0.125
- down_weight: bfloat16 [64, 1024, 2048], P('sp', 'tp'), may hold values from -0.1875 to 0.1875
Outputs:
- output: bfloat16 [16384, 2048], P(('sp', 'tp'))
The draws below stay inside these ranges and needn't reach their ends.
Inputs may be any that keep to these rules, and one draw needn't show every extreme that they name: `expert_ids`: each row names 2 different experts of one group of 16 consecutive numbers; in each aligned block of 128 rows (the rows of one device) no expert is named more than 8 times, and some expert exactly 8 times.
All inputs are finite; a program needn't handle non-finite values.
Results may differ from the reference program's by a relative error of at most 0.013.
Values may be sent and summed in bfloat16 or wider, within the bound.
No kernel may reach another device: no remote copies, remote signals or barrier semaphores. Data moves between devices by JAX's collectives and lax.ppermute only.
A program may use at most 64 MiB of HBM per device.

```python
import math
import jax
import jax.numpy as jnp
import numpy as np
from jax import lax

D = 2048
HEAD_COUNT = 12
UNROTATED_DIM = 64
ROPE = 32
VALUE_ENTRIES = 64
LATENT_RANK = 256
FF = 1024
GROUPS = 4
TOP_K = 2
TOK_DEV = 256
TOKEN_COUNT = 16384
EXPERTS = 64
N_TP = 2


def rope_rows(key):
    drawn = jax.random.normal(jax.random.fold_in(key, 11), (TOKEN_COUNT, ROPE), jnp.float32)
    return jnp.clip(drawn, -6.0, 6.0)


def draw_rope_key(key, part):
    return rope_rows(key).astype(jnp.bfloat16)


def draw_queries(key, part):
    normal_part = jax.random.normal(jax.random.fold_in(key, 12), (TOKEN_COUNT, HEAD_COUNT, UNROTATED_DIM + ROPE), jnp.float32)
    normal_part = jnp.clip(normal_part, -6.0, 6.0)
    return normal_part.reshape(TOKEN_COUNT, HEAD_COUNT * (UNROTATED_DIM + ROPE)).astype(jnp.bfloat16)


def draw_expert_ids(key, part):
    row_count = TOK_DEV // N_TP
    half_rows = row_count // 2
    block_count = TOKEN_COUNT // row_count
    per_group = EXPERTS // GROUPS
    full_group = jax.random.randint(jax.random.fold_in(key, 1), (), 0, GROUPS)
    others = jax.random.randint(jax.random.fold_in(key, 2), (block_count, half_rows), 0, GROUPS - 1)
    others = others + (others >= full_group).astype(jnp.int32)
    group_ids = jnp.concatenate([jnp.full((block_count, half_rows), full_group, jnp.int32), others], axis=1)
    block_keys = jax.random.split(jax.random.fold_in(key, 3), block_count)
    group_ids = jax.vmap(lambda block_key, row_groups: jax.random.permutation(block_key, row_groups))(block_keys, group_ids)
    onehot = (group_ids[..., None] == jnp.arange(GROUPS, dtype=jnp.int32)).astype(jnp.int32)
    earlier = jnp.cumsum(onehot, axis=1) - onehot
    slot_rank = jnp.sum(earlier * onehot, axis=-1)
    offsets = jax.random.randint(jax.random.fold_in(key, 4), (block_count, GROUPS), 0, per_group)
    spacing = jax.random.randint(jax.random.fold_in(key, 5), (block_count, GROUPS), 1, per_group)
    own_offset = jnp.take_along_axis(offsets, group_ids, axis=1)
    own_spacing = jnp.take_along_axis(spacing, group_ids, axis=1)
    first_pick = (slot_rank + own_offset) % per_group
    second_pick = (slot_rank + own_offset + own_spacing) % per_group
    chosen = jnp.stack([group_ids * per_group + first_pick, group_ids * per_group + second_pick], axis=-1)
    return chosen.reshape(TOKEN_COUNT, 2).astype(jnp.int32)


def steps_of(own_key, shape, cuts, least, top_value):
    level, own = 1.0, jax.random.fold_in(own_key, 6)
    for axis_at, blocks in cuts:
        draws = jnp.exp(jax.random.uniform(jax.random.fold_in(own, axis_at), (blocks,), jnp.float32, least / len(cuts), top_value / len(cuts)))
        level = level * jnp.repeat(draws, shape[axis_at] // blocks).reshape([-1 if axis == axis_at else 1 for axis in range(len(shape))])
    return level


def profile(number_of, total, bound, slope):
    weights = [(1 << 20) // math.isqrt(rank ** slope) + 1 for rank in range(2, number_of + 1)]
    spare, counts = total - bound - (number_of - 1), [1] * (number_of - 1)
    while spare > 0:
        free = [i for i in range(number_of - 1) if counts[i] < bound]
        mass, remaining = sum([weights[i] for i in free]), spare
        for i in free:
            extra = min(bound - counts[i], max(1, remaining * weights[i] // mass), spare)
            counts[i] = counts[i] + extra
            spare = spare - extra
    return np.array([bound] + counts)


def uneven_parts(own_key, amount, total, limit, slope):
    if amount == 2:
        one = jax.random.randint(own_key, (), max(1, total - limit), min(limit, total - 1) + 1)
        return jnp.stack([one, total - one])
    tallies = jnp.asarray(profile(amount, total, limit, slope), jnp.int32)
    twos = (amount - 1) // 2
    source_of, sink = tallies[1:1 + 2 * twos:2], tallies[2:2 + 2 * twos:2]
    room = jnp.minimum(source_of - 1, limit - sink)
    moved = jax.random.randint(jax.random.fold_in(own_key, 1), (twos,), 0, 1 << 20) % (room + 1)
    tallies = tallies.at[1:1 + 2 * twos:2].set(source_of - moved).at[2:2 + 2 * twos:2].set(sink + moved)
    return tallies[jax.random.permutation(jax.random.fold_in(own_key, 2), amount)]


def bell_draw(key, extent, scale, most, cuts=(), held_as=jnp.bfloat16):
    values = scale * jax.random.normal(key, extent, jnp.float32)
    if cuts:
        values = values * steps_of(key, extent, cuts, -0.22, 0.18)
    return jnp.clip(values, -most, most).astype(held_as)


def setup_inputs(seed: int = 0) -> dict:
    arg_keys = jax.random.split(jax.random.key(seed), 16)
    return {
        "residual": bell_draw(arg_keys[0], (TOKEN_COUNT, D), 1.0, 6.0, ((0, 128),)),
        "queries": draw_queries(jax.random.fold_in(arg_keys[15], 71), 0),
        "latent": bell_draw(arg_keys[2], (TOKEN_COUNT, LATENT_RANK), 1.0, 6.0, ((0, 64),)),
        "rope_key": draw_rope_key(jax.random.fold_in(arg_keys[15], 71), 0),
        "doc_ids": jnp.searchsorted(jnp.cumsum(uneven_parts(arg_keys[4], 6, TOKEN_COUNT, TOKEN_COUNT // 2, 0)), jnp.arange(TOKEN_COUNT), side="right").astype(jnp.int32),
        "latent_to_key": bell_draw(arg_keys[5], (LATENT_RANK, HEAD_COUNT * UNROTATED_DIM), LATENT_RANK ** -0.5, 0.375, ((1, 2),)),
        "latent_to_value": bell_draw(arg_keys[6], (LATENT_RANK, HEAD_COUNT * VALUE_ENTRIES), LATENT_RANK ** -0.5, 0.375, ((1, 2),)),
        "out_proj": bell_draw(arg_keys[7], (HEAD_COUNT * VALUE_ENTRIES, D), (HEAD_COUNT * VALUE_ENTRIES) ** -0.5, 0.21875),
        "mix_gain": jnp.clip(1.0 + 0.18 * jax.random.normal(arg_keys[8], (D,), jnp.float32), 0.1, 1.9),
        "moe_gain": jnp.clip(1.0 + 0.18 * jax.random.normal(arg_keys[9], (D,), jnp.float32), 0.1, 1.9),
        "expert_ids": draw_expert_ids(jax.random.fold_in(arg_keys[15], 71), 0),
        "route_weight": jnp.clip(0.1 + 0.9 * jax.random.uniform(arg_keys[11], (TOKEN_COUNT, TOP_K), jnp.float32) ** steps_of(arg_keys[11], (TOKEN_COUNT, TOP_K), ((0, 128),), -0.2, 0.2), 0.1, 1.0),
        "gate_weight": bell_draw(arg_keys[12], (EXPERTS, D, FF), D ** -0.5, 0.125, ((0, 64), (2, 2))),
        "up_weight": bell_draw(arg_keys[13], (EXPERTS, D, FF), D ** -0.5, 0.125, ((0, 64), (2, 2))),
        "down_weight": bell_draw(arg_keys[14], (EXPERTS, FF, D), FF ** -0.5, 0.1875, ((0, 64), (1, 2))),
    }


rope_base = 10000.0
epsilon = 1e-06
query_rows = 256

def rotate(source, positions):
    half_width = source.shape[-1] // 2
    frequency = rope_base ** (-jnp.arange(half_width, dtype=jnp.float32) / half_width)
    angles = positions.astype(jnp.float32)[:, None] * frequency[None, :]
    if source.ndim == 3:
        angles = angles[:, None, :]
    cosine = jnp.cos(angles)
    sine_part = jnp.sin(angles)
    upper_half = source[..., :half_width].astype(jnp.float32)
    lower_half = source[..., half_width:].astype(jnp.float32)
    turned = jnp.concatenate([upper_half * cosine - lower_half * sine_part, lower_half * cosine + upper_half * sine_part], axis=-1)
    return turned.astype(jnp.bfloat16)

def rms_scale(source, gain):
    return source * lax.rsqrt(lax.optimization_barrier(jnp.mean(source * source, axis=-1, keepdims=True)) + epsilon) * gain

def reference(residual, queries, latent, rope_key, doc_ids, latent_to_key, latent_to_value, out_proj, mix_gain, moe_gain, expert_ids, route_weight, gate_weight, up_weight, down_weight):
    positions = jnp.arange(TOKEN_COUNT, dtype=jnp.int32)
    key_nope = jnp.dot(latent, latent_to_key, preferred_element_type=jnp.float32).astype(jnp.bfloat16)
    key_nope = key_nope.reshape(TOKEN_COUNT, HEAD_COUNT, UNROTATED_DIM).astype(jnp.float32)
    values = jnp.dot(latent, latent_to_value, preferred_element_type=jnp.float32).astype(jnp.bfloat16)
    values = values.reshape(TOKEN_COUNT, HEAD_COUNT, VALUE_ENTRIES).astype(jnp.float32)
    key_rot = rotate(rope_key, positions).astype(jnp.float32)
    shaped = queries.reshape(TOKEN_COUNT, HEAD_COUNT, UNROTATED_DIM + ROPE)
    query_nope = shaped[..., :UNROTATED_DIM]
    query_rot = rotate(shaped[..., UNROTATED_DIM:], positions)
    score_scale = (UNROTATED_DIM + ROPE) ** (-0.5)
    block_count = TOKEN_COUNT // query_rows

    def attend_rows(bundle):
        nope_block, rot_block, pos_block, doc_block = bundle
        scores = (jnp.einsum('qhd,khd->qhk', nope_block.astype(jnp.float32), key_nope) + jnp.einsum('qhr,kr->qhk', rot_block.astype(jnp.float32), key_rot)) * score_scale
        allowed = ((positions[None, :] <= pos_block[:, None]) & (doc_ids[None, :] == doc_block[:, None]))[:, None, :]
        row_max = lax.optimization_barrier(jnp.max(jnp.where(allowed, scores, -jnp.inf), axis=-1, keepdims=True))
        weights = jnp.where(allowed, jnp.exp(scores - row_max), 0.0)
        totals = lax.optimization_barrier(jnp.sum(weights, axis=-1))
        rounded = lax.optimization_barrier(weights.astype(jnp.bfloat16)).astype(jnp.float32)
        mixed = jnp.einsum('qhk,khd->qhd', rounded, values) / totals[..., None]
        return mixed.astype(jnp.bfloat16).reshape(query_rows, HEAD_COUNT * VALUE_ENTRIES)
    attended = lax.map(attend_rows, (query_nope.reshape(block_count, query_rows, HEAD_COUNT, UNROTATED_DIM), query_rot.reshape(block_count, query_rows, HEAD_COUNT, ROPE), positions.reshape(block_count, query_rows), doc_ids.reshape(block_count, query_rows)))
    attended = attended.reshape(TOKEN_COUNT, HEAD_COUNT * VALUE_ENTRIES)
    mix = jnp.dot(attended, out_proj, preferred_element_type=jnp.float32)
    branch = rms_scale(mix, mix_gain)
    middle = lax.optimization_barrier((residual.astype(jnp.float32) + branch).astype(jnp.bfloat16))
    normed = rms_scale(middle.astype(jnp.float32), moe_gain).astype(jnp.bfloat16)
    row_count = TOK_DEV // N_TP
    groups_blocks = TOKEN_COUNT // row_count
    per_group = EXPERTS // GROUPS
    capacity = row_count // per_group
    flat_ids = expert_ids.reshape(groups_blocks, row_count * TOP_K)
    onehot = (flat_ids[..., None] == jnp.arange(EXPERTS, dtype=jnp.int32)).astype(jnp.int32)
    earlier = jnp.cumsum(onehot, axis=1) - onehot
    slot_rank = lax.optimization_barrier(jnp.sum(earlier * onehot, axis=-1)).astype(jnp.int32)
    block_index = jnp.broadcast_to(jnp.arange(groups_blocks, dtype=jnp.int32)[:, None], flat_ids.shape)
    token_index = (block_index * row_count + jnp.arange(row_count * TOP_K, dtype=jnp.int32)[None, :] // TOP_K).astype(jnp.int32)
    row_table = jnp.full((EXPERTS, groups_blocks, capacity), TOKEN_COUNT, jnp.int32)
    row_table = row_table.at[flat_ids, block_index, slot_rank].set(token_index)
    weight_table = jnp.zeros((EXPERTS, groups_blocks, capacity), jnp.float32)
    weight_table = weight_table.at[flat_ids, block_index, slot_rank].set(route_weight.reshape(groups_blocks, row_count * TOP_K))
    padded = jnp.concatenate([normed, jnp.zeros((1, D), jnp.bfloat16)], axis=0)
    half_units = FF // N_TP

    def expert_step(accumulated, inputs):
        table_rows, table_weights, gate_mat, up_mat, down_mat = inputs
        picked = padded[table_rows.reshape(-1)]
        gate_out = jnp.dot(picked, gate_mat, preferred_element_type=jnp.float32)
        up_out = jnp.dot(picked, up_mat, preferred_element_type=jnp.float32)
        hidden = (jax.nn.silu(gate_out) * up_out).astype(jnp.bfloat16)
        combined = jnp.zeros((picked.shape[0], D), jnp.float32)
        for portion in range(N_TP):
            partial_value = jnp.dot(hidden[:, portion * half_units:(portion + 1) * half_units], down_mat[portion * half_units:(portion + 1) * half_units], preferred_element_type=jnp.float32)
            combined = combined + lax.optimization_barrier(partial_value.astype(jnp.bfloat16)).astype(jnp.float32)
        result = lax.optimization_barrier(combined.astype(jnp.bfloat16)).astype(jnp.float32)
        accumulated = accumulated.at[table_rows.reshape(-1)].add(result * table_weights.reshape(-1)[:, None])
        return (accumulated, None)
    accumulated, _ = lax.scan(expert_step, jnp.zeros((TOKEN_COUNT + 1, D), jnp.float32), (row_table, weight_table, gate_weight, up_weight, down_weight))
    return (middle.astype(jnp.float32) + accumulated[:TOKEN_COUNT]).astype(jnp.bfloat16)
```

```python
import math

import jax
import jax.numpy as jnp
from jax import lax
from jax.experimental import pallas as pl
from jax.experimental.pallas import tpu as pltpu
from jax.sharding import PartitionSpec as P

D = 2048
NOPE = 64
ROPE = 32
HALF = 128
BLOCK = 256
HEADS = 12
LOCAL_HEADS = 6
PLANE = 16
ROWS = 304
CAPACITY = 8
EXPERTS = 64
SLOTS = EXPERTS * CAPACITY
QW = LOCAL_HEADS * 128
KW = 512
VW = 384
PACK = QW + KW + VW
epsilon = 1e-06
LOW = -1e30
SCALE = (NOPE + ROPE) ** -0.5 * math.log2(math.e)
f32 = jnp.float32
bf16 = jnp.bfloat16


def vmem():
    return pl.BlockSpec(memory_space=pltpu.VMEM)


def smem():
    return pl.BlockSpec(memory_space=pltpu.SMEM)


def params(mib=48):
    return pltpu.CompilerParams(vmem_limit_bytes=mib * 1024 * 1024)


def lanes(rows):
    return lax.broadcasted_iota(jnp.int32, (rows, 128), 1)


def turn(x, cosine, sine, lane):
    other = jnp.where(lane < 80, -pltpu.roll(x, 112, 1), pltpu.roll(x, 16, 1))
    return x * cosine + other * sine


def prep_kernel(q_ref, lat_ref, rope_ref, doc_ref, wk_ref, wv_ref, cos_ref, sin_ref, pay_ref, pack_ref):
    half = lax.axis_index("tp")
    lane = lanes(BLOCK)
    cosine, sine = cos_ref[...], sin_ref[...]
    for head in range(LOCAL_HEADS):
        start = head * (NOPE + ROPE)
        panel, off = start // 128, start % 128
        x = q_ref[:, panel * 128 : panel * 128 + 128].astype(f32)
        if off:
            x = pltpu.roll(x, 128 - off, 1)
        if off + NOPE + ROPE > 128:
            width = min(128, q_ref.shape[1] - (panel + 1) * 128)
            y = q_ref[:, (panel + 1) * 128 : (panel + 1) * 128 + width].astype(f32)
            if width < 128:
                y = jnp.concatenate([y, jnp.zeros((BLOCK, 128 - width), f32)], axis=1)
            x = jnp.where(lane < 128 - off, x, pltpu.roll(y, 128 - off, 1))
        x = jnp.where(lane < NOPE + ROPE, x, 0.0)
        pack_ref[:, head * 128 : head * 128 + 128] = turn(x, cosine, sine, lane).astype(bf16)
    w0 = wk_ref[:, 0:128]
    w1 = wk_ref[:, 128:256].astype(f32)
    w2 = wk_ref[:, 256:384].astype(f32)
    r1, r2 = pltpu.roll(w1, 64, 1), pltpu.roll(w2, 64, 1)
    pack_ref[:, QW : QW + 128] = w0
    pack_ref[:, QW + 128 : QW + 256] = jnp.where(lane < 64, w1, 0.0).astype(bf16)
    pack_ref[:, QW + 256 : QW + 384] = jnp.where(lane < 64, r1, r2).astype(bf16)
    pack_ref[:, QW + 384 : QW + 512] = jnp.where(lane < 64, r2, 0.0).astype(bf16)
    pack_ref[:, QW + KW : PACK] = wv_ref[...]
    first = pl.multiple_of(half * HALF, HALF)
    mine = pl.ds(first, HALF)
    pay_ref[0:128, :] = lat_ref[mine, 0:128]
    pay_ref[128:256, :] = lat_ref[mine, 128:256]
    rope = jnp.concatenate([rope_ref[mine, :].astype(f32), jnp.zeros((HALF, 96), f32)], axis=1)
    small = lanes(HALF)
    turned = turn(pltpu.roll(rope, 64, 1), cos_ref[mine, :], sin_ref[mine, :], small)
    turned = jnp.where((small >= 64) & (small < 96), turned, 0.0)
    packed = jnp.zeros((32, 128), f32)
    for c in range(4):
        piece = turned[32 * c : 32 * c + 32, :]
        shift = (32 * c + 64) % 128
        packed = packed + (pltpu.roll(piece, shift, 1) if shift else piece)
    pay_ref[256:288, :] = packed.astype(bf16)
    docs = doc_ref[pl.ds(half, 1), :].astype(f32)
    pay_ref[288:304, :] = jnp.broadcast_to(docs, (16, 128)).astype(bf16)


def attend_kernel(
    arr_ref, ext_ref, own_ref, oth_ref, qdoc_ref, doc_ref, mine_ref, theirs_ref, q_s, k_s, v_s, m_s, l_s, a_s, bias_s, full_s
):
    half = lax.axis_index("tp")
    seat = lax.axis_index("sp")
    plane, spot = seat // PLANE, seat % PLANE
    doc_first = doc_ref[0].astype(f32)
    doc_last = doc_ref[BLOCK - 1].astype(f32)
    lane = lanes(BLOCK)
    for head in range(HEADS):
        src = own_ref if head < LOCAL_HEADS else oth_ref
        local = head % LOCAL_HEADS
        x = src[:, local * 128 : local * 128 + 128].astype(f32)
        if head % 3 == 2:
            lo, hi = jnp.zeros_like(x), x
        else:
            lo, hi = jnp.where(lane < 64, x, 0.0), jnp.where(lane < 64, 0.0, x)
            if head % 3 == 1:
                lo = pltpu.roll(lo, 64, 1)
        q_s[head, :, 0:128] = lo.astype(bf16)
        q_s[head, :, 128:256] = hi.astype(bf16)
    m_s[...] = jnp.full(m_s.shape, LOW, f32)
    l_s[...] = jnp.zeros(l_s.shape, f32)
    a_s[...] = jnp.zeros(a_s.shape, f32)

    def heads(count, masked):
        panels = count // 128
        for head in range(HEADS):
            group = head // 3
            s = lax.dot_general(
                q_s[head],
                k_s[:count, group * 256 : group * 256 + 256],
                (((1,), (1,)), ((), ())),
                preferred_element_type=f32,
            )
            parts = [s[:, 128 * b : 128 * b + 128] for b in range(panels)]
            if masked:
                parts = [part + bias_s[:, 128 * b : 128 * b + 128] for b, part in enumerate(parts)]
            top = parts[0]
            for part in parts[1:]:
                top = jnp.maximum(top, part)
            old = m_s[head]
            new = jnp.maximum(old, jnp.max(top, axis=1, keepdims=True))
            keep = jnp.exp2((old - new) * SCALE)
            weights = [jnp.exp2((part - new) * SCALE) for part in parts]
            total = weights[0]
            for w in weights[1:]:
                total = total + w
            l_s[head] = l_s[head] * keep + total
            m_s[head] = new
            rounded = jnp.concatenate([w.astype(bf16) for w in weights], axis=1) if panels > 1 else weights[0].astype(bf16)
            pair = head // 2
            a_s[head] = a_s[head] * keep + jnp.dot(
                rounded, v_s[:count, pair * 128 : pair * 128 + 128], preferred_element_type=f32
            )

    def tile(load, bases, own_flags):
        panels = len(bases)
        count = panels * 128
        rows = [load(b, 288, 304).astype(f32) for b in range(panels)]
        seen = [jnp.where(base >= 0, row, -1.0) for base, row in zip(bases, rows)]
        high, low = seen[0], seen[0]
        for row in seen[1:]:
            high, low = jnp.maximum(high, row), jnp.minimum(low, row)
        high, low = jnp.max(high), jnp.min(low)
        has_own = own_flags[0]
        for flag in own_flags[1:]:
            has_own = has_own | flag
        active = high >= doc_first
        plain = (low == doc_last) & jnp.logical_not(has_own)

        @pl.when(active)
        def _():
            lat = jnp.concatenate(
                [
                    jnp.concatenate([load(b, 0, 128) for b in range(panels)], axis=0),
                    jnp.concatenate([load(b, 128, 256) for b in range(panels)], axis=0),
                ],
                axis=1,
            )
            turned = []
            for b in range(panels):
                r = load(b, 256, 288).astype(f32)
                turned += [pltpu.roll(r, 64, 1), pltpu.roll(r, 32, 1), r, pltpu.roll(r, 96, 1)]
            turned = jnp.concatenate(turned, axis=0)
            wide = lanes(count)
            turned = jnp.where((wide >= 64) & (wide < 96), turned, 0.0)
            for side, src in enumerate((own_ref, oth_ref)):
                keys = jnp.dot(lat, src[:, QW : QW + KW], preferred_element_type=f32)
                for g in range(2):
                    at = side * 512 + g * 256
                    k_s[:count, at : at + 128] = keys[:, g * 256 : g * 256 + 128].astype(bf16)
                    k_s[:count, at + 128 : at + 256] = (keys[:, g * 256 + 128 : g * 256 + 256] + turned).astype(bf16)
                v_s[:count, side * 384 : side * 384 + 384] = jnp.dot(
                    lat, src[:, QW + KW : PACK], preferred_element_type=f32
                ).astype(bf16)

        @pl.when(active & plain)
        def _():
            heads(count, False)

        @pl.when(active & jnp.logical_not(plain))
        def _():
            at_query = seat * BLOCK + lax.broadcasted_iota(jnp.int32, (BLOCK, 128), 0)
            for b in range(panels):
                at_key = jnp.where(bases[b] >= 0, bases[b], 1 << 20) + lane
                allowed = (at_key <= at_query) & (rows[b][0:1, :] == qdoc_ref[...])
                bias_s[:, 128 * b : 128 * b + 128] = jnp.where(allowed, 0.0, LOW)
            heads(count, True)

    def place(block):
        return jnp.where(block >= 0, block * BLOCK + half * HALF, -1)

    tile(lambda b, lo, hi: ext_ref[lo:hi, :], [place((plane - 2) * PLANE + spot)], [jnp.bool_(False)])

    def step(number, carried):
        kind, quad = number // 4, number % 4
        bases, flags = [], []
        for b in range(4):
            i = quad * 4 + b
            late = (plane - jnp.where(i <= spot, 0, 2)) * PLANE + i
            block = jnp.where(kind == 0, (plane - 1) * PLANE + i, late)
            bases.append(place(block))
            flags.append(block == seat)
        tile(lambda b, lo, hi: arr_ref[quad * 4 + b, kind, lo:hi, :], bases, flags)
        return carried

    lax.fori_loop(0, 8, step, 0)

    stats = jnp.zeros((BLOCK, 128), f32)
    for head in range(HEADS):
        at = head + jnp.where(half == 0, 0, LOCAL_HEADS if head < LOCAL_HEADS else -LOCAL_HEADS)
        stats = jnp.where(lane == at, m_s[head], stats)
        stats = jnp.where(lane == at + 16, jnp.sum(l_s[head], axis=1, keepdims=True), stats)
    full_s[:, 768:896] = stats
    for pair in range(6):
        both = jnp.where(lane < 64, a_s[2 * pair], a_s[2 * pair + 1])

        @pl.when(half == 0)
        def _():
            full_s[:, pair * 128 : pair * 128 + 128] = both

        @pl.when(half == 1)
        def _():
            at = (pair + 3) % 6
            full_s[:, at * 128 : at * 128 + 128] = both

    mine_ref[...] = full_s[pl.ds(pl.multiple_of(half * HALF, HALF), HALF), :]
    theirs_ref[...] = full_s[pl.ds(pl.multiple_of((1 - half) * HALF, HALF), HALF), :]


def slots_of(ids):
    expert = lax.broadcasted_iota(jnp.int32, (HALF, EXPERTS), 1)
    named = [(ids[:, k : k + 1] == expert) for k in range(2)]
    counts = named[0].astype(f32) + named[1].astype(f32)
    row = lax.broadcasted_iota(jnp.int32, (HALF, HALF), 0)
    col = lax.broadcasted_iota(jnp.int32, (HALF, HALF), 1)
    earlier = jnp.dot((col < row).astype(f32).astype(bf16), counts.astype(bf16), preferred_element_type=f32)
    slot = lax.broadcasted_iota(jnp.int32, (HALF, SLOTS), 1)
    picks = []
    for k in range(2):
        rank = jnp.sum(jnp.where(named[k], earlier, 0.0), axis=1, keepdims=True)
        at = ids[:, k : k + 1] * CAPACITY + rank.astype(jnp.int32)
        picks.append((slot == at).astype(f32).astype(bf16))
    return picks


def norm_of(x):
    return lax.rsqrt(jnp.mean(x * x, axis=-1, keepdims=True) + epsilon)


def mix_kernel(mine_ref, theirs_ref, proj_ref, res_ref, mixg_ref, moeg_ref, ids_ref, mid_ref, buf_ref):
    lane = lanes(HALF)
    sm, st = mine_ref[:, 768:896], theirs_ref[:, 768:896]
    top = jnp.maximum(sm, st)
    wm = jnp.exp2((sm - top) * SCALE)
    wt = jnp.exp2((st - top) * SCALE)
    panels = []
    for pair in range(6):
        fm, ft, total = [], [], []
        for head in (2 * pair, 2 * pair + 1):
            a, b = wm[:, head : head + 1], wt[:, head : head + 1]
            fm.append(a)
            ft.append(b)
            total.append(a * sm[:, 16 + head : 17 + head] + b * st[:, 16 + head : 17 + head])
        cols = slice(pair * 128, pair * 128 + 128)
        value = mine_ref[:, cols] * jnp.where(lane < 64, fm[0], fm[1]) + theirs_ref[:, cols] * jnp.where(lane < 64, ft[0], ft[1])
        panels.append((value / jnp.where(lane < 64, total[0], total[1])).astype(bf16))
    attended = jnp.concatenate(panels, axis=1)
    mix = jnp.dot(attended, proj_ref[...], preferred_element_type=f32)
    branch = mix * norm_of(mix) * mixg_ref[...]
    middle = (res_ref[...].astype(f32) + branch).astype(bf16)
    mid_ref[...] = middle
    wide = middle.astype(f32)
    normed = (wide * norm_of(wide) * moeg_ref[...]).astype(bf16)
    picks = slots_of(ids_ref[...])
    buf_ref[...] = lax.dot_general(
        picks[0] + picks[1], normed, (((0,), (0,)), ((), ())), preferred_element_type=f32
    ).astype(bf16)


def pick_kernel(back_ref, mid_ref, ids_ref, weight_ref, out_ref):
    picks = slots_of(ids_ref[...])
    total = mid_ref[...].astype(f32)
    for k in range(2):
        rows = jnp.dot(picks[k], back_ref[...], preferred_element_type=f32)
        total = total + rows * weight_ref[:, k : k + 1]
    out_ref[...] = total.astype(bf16)


def local(
    residual,
    queries,
    latent,
    rope_key,
    doc_ids,
    latent_to_key,
    latent_to_value,
    out_proj,
    mix_gain,
    moe_gain,
    expert_ids,
    route_weight,
    gate_weight,
    up_weight,
    down_weight,
):
    sp = lax.axis_size("sp")
    seat = lax.axis_index("sp")
    spot = seat % PLANE
    swap = [(0, 1), (1, 0)]
    lane = jnp.arange(128, dtype=jnp.int32)
    frequency = jnp.where(
        (lane >= 64) & (lane < 96), 10000.0 ** (-(lane % 16).astype(f32) / 16), 0.0
    )
    positions = seat * BLOCK + jnp.arange(BLOCK, dtype=jnp.int32)
    angles = positions.astype(f32)[:, None] * frequency[None, :]
    payload, pack = pl.pallas_call(
        prep_kernel,
        out_shape=(jax.ShapeDtypeStruct((ROWS, 128), bf16), jax.ShapeDtypeStruct((BLOCK, PACK), bf16)),
        in_specs=[vmem()] * 8,
        out_specs=(vmem(), vmem()),
        compiler_params=params(),
        name="prep",
    )(queries, latent, rope_key, doc_ids.reshape(2, 128), latent_to_key, latent_to_value, jnp.cos(angles), jnp.sin(angles))
    before = [lax.ppermute(payload, "sp", [(i, i + PLANE * k) for i in range(sp - PLANE * k)]) for k in (1, 2)]
    other = lax.ppermute(pack, "tp", swap)
    target = jnp.arange(PLANE, dtype=jnp.int32)[:, None, None]
    sent = jnp.stack(
        [jnp.broadcast_to(before[0][None], (PLANE, ROWS, 128)), jnp.where(spot <= target, payload[None], before[1][None])],
        axis=1,
    )
    groups = [[z * PLANE + i for i in range(PLANE)] for z in range(sp // PLANE)]
    arrived = lax.all_to_all(sent, "sp", 0, 0, axis_index_groups=groups, tiled=True)
    query_docs = jnp.broadcast_to(doc_ids.astype(f32)[:, None], (BLOCK, 128))
    stat = jax.ShapeDtypeStruct((HALF, 896), f32)
    mine, theirs = pl.pallas_call(
        attend_kernel,
        out_shape=(stat, stat),
        in_specs=[vmem()] * 5 + [smem()],
        out_specs=(vmem(), vmem()),
        scratch_shapes=[
            pltpu.VMEM((HEADS, BLOCK, 256), bf16),
            pltpu.VMEM((512, 1024), bf16),
            pltpu.VMEM((512, 768), bf16),
            pltpu.VMEM((HEADS, BLOCK, 128), f32),
            pltpu.VMEM((HEADS, BLOCK, 128), f32),
            pltpu.VMEM((HEADS, BLOCK, 128), f32),
            pltpu.VMEM((BLOCK, 512), f32),
            pltpu.VMEM((BLOCK, 896), f32),
        ],
        compiler_params=params(),
        name="attend",
    )(arrived, before[1], pack, other, query_docs, doc_ids)
    theirs = lax.ppermute(theirs, "tp", swap)
    middle, buffer = pl.pallas_call(
        mix_kernel,
        out_shape=(jax.ShapeDtypeStruct((HALF, D), bf16), jax.ShapeDtypeStruct((SLOTS, D), bf16)),
        in_specs=[vmem()] * 7,
        out_specs=(vmem(), vmem()),
        compiler_params=params(),
        name="mix",
    )(mine, theirs, out_proj, residual, mix_gain[None], moe_gain[None], expert_ids)
    rows = lax.all_to_all(buffer.reshape(EXPERTS, CAPACITY, D), "sp", 0, 0, tiled=True).reshape(SLOTS, D)
    own = (gate_weight[0], up_weight[0], down_weight[0])
    swapped = tuple(lax.ppermute(w, "tp", swap) for w in own)
    result = 0.0
    for gate, up, down in (own, swapped):
        gated = jnp.dot(rows, gate, preferred_element_type=f32)
        upward = jnp.dot(rows, up, preferred_element_type=f32)
        hidden = (jax.nn.silu(gated) * upward).astype(bf16)
        part = lax.optimization_barrier(jnp.dot(hidden, down, preferred_element_type=f32).astype(bf16))
        result = result + part.astype(f32)
    result = result.astype(bf16).reshape(EXPERTS, CAPACITY, D)
    back = lax.all_to_all(result, "sp", 0, 0, tiled=True).reshape(SLOTS, D)
    return pl.pallas_call(
        pick_kernel,
        out_shape=jax.ShapeDtypeStruct((HALF, D), bf16),
        in_specs=[vmem()] * 4,
        out_specs=vmem(),
        compiler_params=params(),
        name="pick",
    )(back, middle, expert_ids, route_weight)


def solution(mesh):
    in_specs = (
        P(("sp", "tp"), None),
        P("sp", "tp"),
        P("sp", None),
        P("sp", None),
        P("sp"),
        P(None, "tp"),
        P(None, "tp"),
        P(),
        P(),
        P(),
        P(("sp", "tp"), None),
        P(("sp", "tp"), None),
        P("sp", None, "tp"),
        P("sp", None, "tp"),
        P("sp", "tp", None),
    )
    out_specs = P(("sp", "tp"), None)
    return jax.shard_map(local, mesh=mesh, in_specs=in_specs, out_specs=out_specs, check_vma=False)
```

```python
import functools
import math

import jax
import jax.numpy as jnp
from jax import lax
from jax.experimental import pallas as pl
from jax.experimental.pallas import tpu as pltpu
from jax.sharding import PartitionSpec as P

D = 2048
NOPE = 64
ROPE = 32
HALF = 128
BLOCK = 256
HEADS = 12
LOCAL_HEADS = 6
PLANE = 16
ROWS = 304
CAPACITY = 8
EXPERTS = 64
SLOTS = EXPERTS * CAPACITY
QW = LOCAL_HEADS * 128
KW = 512
VW = 384
PACK = QW + KW + VW
epsilon = 1e-06
ATTEND_MIB = 24
LOW = -1e30
SCALE = (NOPE + ROPE) ** -0.5 * math.log2(math.e)
f32 = jnp.float32
bf16 = jnp.bfloat16


def vmem():
    return pl.BlockSpec(memory_space=pltpu.VMEM)


def smem():
    return pl.BlockSpec(memory_space=pltpu.SMEM)


def hbm():
    return pl.BlockSpec(memory_space=pltpu.HBM)


def far(x):
    return pltpu.with_memory_space_constraint(x, pltpu.HBM)


def params(mib):
    return pltpu.CompilerParams(vmem_limit_bytes=mib * 1024 * 1024)


def lanes(rows):
    return lax.broadcasted_iota(jnp.int32, (rows, 128), 1)


def turn(first, second, cosine, sine):
    return first * cosine - second * sine, second * cosine + first * sine


def prep_kernel(*refs):
    inputs, (pay_ref, pack_ref) = refs[:8], refs[8:10]
    held, sems = refs[10:18], refs[18]
    copies = [pltpu.make_async_copy(src, dst, sems.at[i]) for i, (src, dst) in enumerate(zip(inputs, held))]
    for copy in copies:
        copy.start()
    for copy in copies:
        copy.wait()
    q_ref, lat_ref, rope_ref, doc_ref, wk_ref, wv_ref, cos_ref, sin_ref = held
    half = lax.axis_index("tp")
    cosine, sine = cos_ref[...], sin_ref[...]
    mine = pl.ds(pl.multiple_of(half * HALF, HALF), HALF)
    pay_ref[0:128, :] = lat_ref[mine, 0:128]
    pay_ref[128:256, :] = lat_ref[mine, 128:256]
    rope = rope_ref[...].astype(f32)
    turned = jnp.concatenate(turn(rope[:16], rope[16:], cosine, sine), axis=0)
    turned = jnp.where(half == 0, turned[:, :128], turned[:, 128:])
    turned = jnp.concatenate([turned, jnp.zeros((96, 128), f32)], axis=0).T
    packed = turned[0:32, :]
    for c in range(1, 4):
        packed = packed + pltpu.roll(turned[32 * c : 32 * c + 32, :], 32 * c, 1)
    pay_ref[256:288, :] = packed.astype(bf16)
    docs = doc_ref[pl.ds(half, 1), :].astype(f32)
    pay_ref[288:304, :] = jnp.broadcast_to(docs, (16, 128)).astype(bf16)
    lane = lanes(BLOCK)
    for head in range(LOCAL_HEADS):
        start = head * (NOPE + ROPE)
        plain = q_ref[start : start + NOPE, :].astype(f32)
        rot = q_ref[start + NOPE : start + NOPE + ROPE, :].astype(f32)
        x = jnp.concatenate([plain, *turn(rot[:16], rot[16:], cosine, sine), jnp.zeros((32, BLOCK), f32)], axis=0)
        pack_ref[:, head * 128 : head * 128 + 128] = x.T.astype(bf16)
    w0 = wk_ref[:, 0:128]
    w1 = wk_ref[:, 128:256].astype(f32)
    w2 = wk_ref[:, 256:384].astype(f32)
    r1, r2 = pltpu.roll(w1, 64, 1), pltpu.roll(w2, 64, 1)
    pack_ref[:, QW : QW + 128] = w0
    pack_ref[:, QW + 128 : QW + 256] = jnp.where(lane < 64, w1, 0.0).astype(bf16)
    pack_ref[:, QW + 256 : QW + 384] = jnp.where(lane < 64, r1, r2).astype(bf16)
    pack_ref[:, QW + 384 : QW + 512] = jnp.where(lane < 64, r2, 0.0).astype(bf16)
    pack_ref[:, QW + KW : PACK] = wv_ref[...]


def spread_kernel(own_ref, oth_ref, q_ref):
    lane = lanes(BLOCK)
    for head in range(HEADS):
        src = own_ref if head < LOCAL_HEADS else oth_ref
        local = head % LOCAL_HEADS
        x = src[:, local * 128 : local * 128 + 128].astype(f32)
        if head % 3 == 2:
            lo, hi = jnp.zeros_like(x), x
        else:
            lo, hi = jnp.where(lane < 64, x, 0.0), jnp.where(lane < 64, 0.0, x)
            if head % 3 == 1:
                lo = pltpu.roll(lo, 64, 1)
        q_ref[head, :, 0:128] = lo.astype(bf16)
        q_ref[head, :, 128:256] = hi.astype(bf16)


def attend_kernel(late, *refs):
    if late:
        ext_ref, refs = refs[0], refs[1:]
    src_ref, q_ref, own_ref, oth_ref, qdoc_ref, doc_ref, mine_ref, theirs_ref = refs[:8]
    k_s, v_s, m_s, a_s, bias_s, full_s, arr_ref, sem = refs[8:]
    fetch = pltpu.make_async_copy(src_ref, arr_ref, sem)
    fetch.start()
    half = lax.axis_index("tp")
    seat = lax.axis_index("sp")
    plane, spot = seat // PLANE, seat % PLANE
    doc_first = doc_ref[0].astype(f32)
    doc_last = doc_ref[BLOCK - 1].astype(f32)
    lane = lanes(BLOCK)
    m_s[...] = jnp.full(m_s.shape, LOW, f32)
    a_s[...] = jnp.zeros(a_s.shape, f32)
    fetch.wait()

    def block_of(i):
        if not late:
            return (plane - 1) * PLANE + i
        return (plane - jnp.where(i <= spot, 0, 2)) * PLANE + i

    def place(block):
        return jnp.where(block >= 0, block * BLOCK + half * HALF, -1)

    groups = [[(arr_ref, 8 * t + b, block_of(8 * t + b)) for b in range(8)] for t in range(2)]
    if late:
        groups.append([(ext_ref, None, (plane - 2) * PLANE + spot)])
    row_lane = lax.broadcasted_iota(jnp.int32, (1, 128), 1)
    code = jnp.zeros((1, 128), f32)
    for t, group in enumerate(groups):
        high = low = None
        for ref, i, block in group:
            docs = (ref[288:304, :] if i is None else ref[i, 288:304, :]).astype(f32)[0:1, :]
            seen = jnp.where(block >= 0, docs, -1.0)
            bound = jnp.where(block == seat, -1.0, seen)
            high = seen if high is None else jnp.maximum(high, seen)
            low = bound if low is None else jnp.minimum(low, bound)
        code = code + jnp.where((row_lane == 127) & (high >= doc_first), float(2 ** (2 * t)), 0.0)
        code = code + jnp.where((row_lane == 0) & (low == doc_last), float(2 ** (2 * t + 1)), 0.0)
    code = jnp.sum(code).astype(jnp.int32)

    def heads(count, masked):
        panels = count // 128

        def side(number, carried):
            first = number * LOCAL_HEADS

            def score(head):
                return lax.dot_general(
                    q_ref[first + head],
                    k_s[2 * number + head // 3, :count, :],
                    (((1,), (1,)), ((), ())),
                    preferred_element_type=f32,
                )

            following = score(0)
            for head in range(LOCAL_HEADS):
                s = following
                if head + 1 < LOCAL_HEADS:
                    following = score(head + 1)
                at = first + head
                parts = [s[:, 128 * b : 128 * b + 128] for b in range(panels)]
                if masked:
                    parts = [part + bias_s[:, 128 * b : 128 * b + 128] for b, part in enumerate(parts)]
                top = parts[0]
                for part in parts[1:]:
                    top = jnp.maximum(top, part)
                old = m_s[at]
                new = jnp.maximum(old, jnp.max(top, axis=1, keepdims=True))
                keep = jnp.exp2((old - new) * SCALE)
                m_s[at] = new
                weights = [jnp.exp2((part - new) * SCALE).astype(bf16) for part in parts]
                rounded = jnp.concatenate(weights, axis=1) if panels > 1 else weights[0]
                a_s[at] = a_s[at] * keep + jnp.dot(rounded, v_s[at, :count, :], preferred_element_type=f32)
            return carried

        lax.fori_loop(0, 2, side, 0)

    def tile(load, blocks, flags):
        panels = len(blocks)
        count = panels * 128
        active = (flags & 1) == 1
        plain = (flags & 2) == 2

        @pl.when(active)
        def _():
            lat = jnp.concatenate(
                [
                    jnp.concatenate([load(b, 0, 128) for b in range(panels)], axis=0),
                    jnp.concatenate([load(b, 128, 256) for b in range(panels)], axis=0),
                ],
                axis=1,
            )
            turned = []
            for b in range(panels):
                r = load(b, 256, 288).astype(f32)
                turned += [pltpu.roll(r, 64, 1), pltpu.roll(r, 32, 1), r, pltpu.roll(r, 96, 1)]
            turned = jnp.concatenate(turned, axis=0)
            wide = lanes(count)
            turned = jnp.where((wide >= 64) & (wide < 96), turned, 0.0)
            for side, src in enumerate((own_ref, oth_ref)):
                keys = jnp.dot(lat, src[:, QW : QW + KW], preferred_element_type=f32)
                for g in range(2):
                    at = side * 2 + g
                    k_s[at, :count, 0:128] = keys[:, g * 256 : g * 256 + 128].astype(bf16)
                    k_s[at, :count, 128:256] = (keys[:, g * 256 + 128 : g * 256 + 256] + turned).astype(bf16)
                rows = jnp.dot(lat, src[:, QW + KW : PACK], preferred_element_type=f32)
                for pair in range(3):
                    both = rows[:, pair * 128 : pair * 128 + 128]
                    at = side * LOCAL_HEADS + pair * 2
                    v_s[at, :count, :] = jnp.where(wide < 64, both, 1.0).astype(bf16)
                    v_s[at + 1, :count, :] = jnp.where(wide < 64, 1.0, both).astype(bf16)

        if panels > 1:

            @pl.when(active & plain)
            def _():
                heads(count, False)

        @pl.when(active & jnp.logical_not(plain) if panels > 1 else active)
        def _():
            at_query = seat * BLOCK + lax.broadcasted_iota(jnp.int32, (BLOCK, 128), 0)
            for b in range(panels):
                base = place(blocks[b])
                at_key = jnp.where(base >= 0, base, 1 << 20) + lane
                docs = load(b, 288, 304).astype(f32)[0:1, :]
                allowed = (at_key <= at_query) & (docs == qdoc_ref[...])
                bias_s[:, 128 * b : 128 * b + 128] = jnp.where(allowed, 0.0, LOW)
            heads(count, True)

    if late:
        tile(lambda b, lo, hi: ext_ref[lo:hi, :], [groups[2][0][2]], code >> 4)

    def step(number, carried):
        blocks = [block_of(number * 8 + b) for b in range(8)]
        tile(lambda b, lo, hi: arr_ref[number * 8 + b, lo:hi, :], blocks, code >> (2 * number))
        return carried

    lax.fori_loop(0, 2, step, 0)

    stats = jnp.zeros((BLOCK, 128), f32)
    for head in range(HEADS):
        at = head + jnp.where(half == 0, 0, LOCAL_HEADS if head < LOCAL_HEADS else -LOCAL_HEADS)
        stats = jnp.where(lane == at, m_s[head], stats)
        spare = 64 if head % 2 == 0 else 0
        stats = jnp.where(lane == at + 16, a_s[head, :, spare : spare + 1], stats)
    full_s[:, 768:896] = stats
    for pair in range(6):
        both = jnp.where(lane < 64, a_s[2 * pair], a_s[2 * pair + 1])

        @pl.when(half == 0)
        def _():
            full_s[:, pair * 128 : pair * 128 + 128] = both

        @pl.when(half == 1)
        def _():
            at = (pair + 3) % 6
            full_s[:, at * 128 : at * 128 + 128] = both

    mine_ref[...] = full_s[pl.ds(pl.multiple_of(half * HALF, HALF), HALF), :]
    theirs_ref[...] = full_s[pl.ds(pl.multiple_of((1 - half) * HALF, HALF), HALF), :]


def slots_of(ids):
    expert = lax.broadcasted_iota(jnp.int32, (EXPERTS, HALF), 0)
    named = [(ids[k : k + 1, :] == expert) for k in range(2)]
    counts = named[0].astype(f32) + named[1].astype(f32)
    row = lax.broadcasted_iota(jnp.int32, (HALF, HALF), 0)
    col = lax.broadcasted_iota(jnp.int32, (HALF, HALF), 1)
    earlier = jnp.dot(counts.astype(bf16), (row < col).astype(f32).astype(bf16), preferred_element_type=f32)
    slot = lax.broadcasted_iota(jnp.int32, (SLOTS, HALF), 0)
    picks = []
    for k in range(2):
        rank = jnp.sum(jnp.where(named[k], earlier, 0.0), axis=0, keepdims=True)
        at = ids[k : k + 1, :] * CAPACITY + rank.astype(jnp.int32)
        picks.append((slot == at).astype(f32).astype(bf16))
    return picks


def norm_of(x):
    return lax.rsqrt(jnp.mean(x * x, axis=-1, keepdims=True) + epsilon)


def mix_kernel(*refs):
    parts, (proj_ref, res_ref, mixg_ref, moeg_ref, ids_ref, mid_ref, buf_ref) = refs[:4], refs[4:]
    lane = lanes(HALF)
    stats = [part[:, 768:896] for part in parts]
    top = jnp.maximum(jnp.maximum(stats[0], stats[1]), jnp.maximum(stats[2], stats[3]))
    shares = [jnp.exp2((s - top) * SCALE) for s in stats]
    panels = []
    for pair in range(6):
        cols = slice(pair * 128, pair * 128 + 128)
        value, total = 0.0, 0.0
        for part, s, share in zip(parts, stats, shares):
            even, odd = share[:, 2 * pair : 2 * pair + 1], share[:, 2 * pair + 1 : 2 * pair + 2]
            scale = jnp.where(lane < 64, even, odd)
            value = value + part[:, cols] * scale
            total = total + scale * jnp.where(lane < 64, s[:, 16 + 2 * pair : 17 + 2 * pair], s[:, 17 + 2 * pair : 18 + 2 * pair])
        panels.append((value / total).astype(bf16))
    attended = jnp.concatenate(panels, axis=1)
    mix = jnp.dot(attended, proj_ref[...], preferred_element_type=f32)
    branch = mix * norm_of(mix) * mixg_ref[...]
    middle = (res_ref[...].astype(f32) + branch).astype(bf16)
    mid_ref[...] = middle
    wide = middle.astype(f32)
    normed = (wide * norm_of(wide) * moeg_ref[...]).astype(bf16)
    picks = slots_of(ids_ref[...])
    buf_ref[...] = jnp.dot(picks[0] + picks[1], normed, preferred_element_type=f32).astype(bf16)


def expert_kernel(rows_ref, *refs):
    weights, out_ref, held, first_s, sems = refs[:6], refs[6], refs[7:13], refs[13], refs[14]
    copies = [pltpu.make_async_copy(src, dst, sems.at[i]) for i, (src, dst) in enumerate(zip(weights, held))]
    for copy in copies:
        copy.start()
    rows = rows_ref[...]
    for side in range(2):
        gate, up, down = held[3 * side : 3 * side + 3]
        copies[3 * side].wait()
        gated = jnp.dot(rows, gate[...], preferred_element_type=f32)
        copies[3 * side + 1].wait()
        upward = jnp.dot(rows, up[...], preferred_element_type=f32)
        hidden = (gated / (1.0 + jnp.exp(-gated)) * upward).astype(bf16)
        copies[3 * side + 2].wait()
        part = jnp.dot(hidden, down[...], preferred_element_type=f32).astype(bf16)
        if side == 0:
            first_s[...] = part
        else:
            out_ref[...] = (first_s[...].astype(f32) + part.astype(f32)).astype(bf16)


def pick_kernel(back_ref, mid_ref, ids_ref, weight_ref, out_ref):
    picks = slots_of(ids_ref[...])
    total = mid_ref[...].astype(f32)
    for k in range(2):
        rows = lax.dot_general(picks[k], back_ref[...], (((0,), (0,)), ((), ())), preferred_element_type=f32)
        column = jnp.broadcast_to(weight_ref[k : k + 1, :], (HALF, HALF)).T
        total = total + rows * column[:, 0:1]
    out_ref[...] = total.astype(bf16)


def local(
    residual,
    queries,
    latent,
    rope_key,
    doc_ids,
    latent_to_key,
    latent_to_value,
    out_proj,
    mix_gain,
    moe_gain,
    expert_ids,
    route_weight,
    gate_weight,
    up_weight,
    down_weight,
):
    sp = lax.axis_size("sp")
    seat = lax.axis_index("sp")
    spot = seat % PLANE
    swap = [(0, 1), (1, 0)]
    frequency = 10000.0 ** (-jnp.arange(16, dtype=f32) / 16)
    positions = seat * BLOCK + jnp.arange(BLOCK, dtype=jnp.int32)
    angles = positions.astype(f32)[None, :] * frequency[:, None]
    inputs = (queries.T, latent, rope_key.T, doc_ids.reshape(2, 128), latent_to_key, latent_to_value, jnp.cos(angles), jnp.sin(angles))
    payload, pack = pl.pallas_call(
        prep_kernel,
        out_shape=(jax.ShapeDtypeStruct((ROWS, 128), bf16), jax.ShapeDtypeStruct((BLOCK, PACK), bf16)),
        in_specs=[hbm()] * 8,
        out_specs=(vmem(), vmem()),
        scratch_shapes=[pltpu.VMEM(x.shape, x.dtype) for x in inputs] + [pltpu.SemaphoreType.DMA((8,))],
        compiler_params=params(8),
        name="prep",
    )(*map(far, inputs))
    before = [lax.ppermute(payload, "sp", [(i, i + PLANE * k) for i in range(sp - PLANE * k)]) for k in (1, 2)]
    other = lax.ppermute(pack, "tp", swap)
    target = jnp.arange(PLANE, dtype=jnp.int32)[:, None, None]
    groups = [[z * PLANE + i for i in range(PLANE)] for z in range(sp // PLANE)]
    late = lax.all_to_all(
        jnp.where(spot <= target, payload[None], before[1][None]), "sp", 0, 0, axis_index_groups=groups, tiled=True
    )
    early = lax.all_to_all(
        jnp.broadcast_to(before[0][None], (PLANE, ROWS, 128)), "sp", 0, 0, axis_index_groups=groups, tiled=True
    )
    query_docs = jnp.broadcast_to(doc_ids.astype(f32)[:, None], (BLOCK, 128))
    spread = pl.pallas_call(
        spread_kernel,
        out_shape=jax.ShapeDtypeStruct((HEADS, BLOCK, 256), bf16),
        in_specs=[vmem()] * 2,
        out_specs=vmem(),
        compiler_params=params(6),
        name="spread",
    )(pack, other)
    stat = jax.ShapeDtypeStruct((HALF, 896), f32)

    def attend(is_late, *operands):
        mine, theirs = pl.pallas_call(
            functools.partial(attend_kernel, is_late),
            out_shape=(pltpu.HBM((HALF, 896), f32),) * 2 if is_late else (stat, stat),
            in_specs=[vmem()] * (len(operands) - 1) + [hbm()] + [vmem()] * 4 + [smem()],
            out_specs=(vmem(), vmem()),
            scratch_shapes=[
                pltpu.VMEM((4, 1024, 256), bf16),
                pltpu.VMEM((HEADS, 1024, 128), bf16),
                pltpu.VMEM((HEADS, BLOCK, 128), f32),
                pltpu.VMEM((HEADS, BLOCK, 128), f32),
                pltpu.VMEM((BLOCK, 1024), f32),
                pltpu.VMEM((BLOCK, 896), f32),
                pltpu.VMEM((PLANE, ROWS, 128), bf16),
                pltpu.SemaphoreType.DMA(()),
            ],
            compiler_params=params(ATTEND_MIB),
            name="attend_late" if is_late else "attend_early",
        )(*operands[:-1], far(operands[-1]), spread, pack, other, query_docs, doc_ids)
        return mine, lax.ppermute(theirs, "tp", swap)

    parts = attend(True, before[1], late) + attend(False, early)
    middle, buffer = pl.pallas_call(
        mix_kernel,
        out_shape=(jax.ShapeDtypeStruct((HALF, D), bf16), pltpu.HBM((SLOTS, D), bf16)),
        in_specs=[vmem()] * 9,
        out_specs=(vmem(), vmem()),
        compiler_params=params(16),
        name="mix",
    )(*parts, out_proj, residual, mix_gain[None], moe_gain[None], expert_ids.T)
    rows = lax.all_to_all(buffer.reshape(EXPERTS, CAPACITY, D), "sp", 0, 0, tiled=True).reshape(SLOTS, D)
    own = (gate_weight[0], up_weight[0], down_weight[0])
    swapped = tuple(lax.ppermute(w, "tp", swap) for w in own)
    result = pl.pallas_call(
        expert_kernel,
        out_shape=jax.ShapeDtypeStruct((SLOTS, D), bf16),
        in_specs=[vmem()] + [hbm()] * 6,
        out_specs=vmem(),
        scratch_shapes=[pltpu.VMEM(w.shape, bf16) for w in own * 2]
        + [pltpu.VMEM((SLOTS, D), bf16), pltpu.SemaphoreType.DMA((6,))],
        compiler_params=params(32),
        name="experts",
    )(rows, *map(far, own + swapped)).reshape(EXPERTS, CAPACITY, D)
    back = lax.all_to_all(result, "sp", 0, 0, tiled=True).reshape(SLOTS, D)
    return pl.pallas_call(
        pick_kernel,
        out_shape=jax.ShapeDtypeStruct((HALF, D), bf16),
        in_specs=[vmem()] * 4,
        out_specs=vmem(),
        compiler_params=params(10),
        name="pick",
    )(back, middle, expert_ids.T, route_weight.T)


def solution(mesh):
    in_specs = (
        P(("sp", "tp"), None),
        P("sp", "tp"),
        P("sp", None),
        P("sp", None),
        P("sp"),
        P(None, "tp"),
        P(None, "tp"),
        P(),
        P(),
        P(),
        P(("sp", "tp"), None),
        P(("sp", "tp"), None),
        P("sp", None, "tp"),
        P("sp", None, "tp"),
        P("sp", "tp", None),
    )
    out_specs = P(("sp", "tp"), None)
    return jax.shard_map(local, mesh=mesh, in_specs=in_specs, out_specs=out_specs, check_vma=False)
```

```python
import functools
import math

import jax
import jax.numpy as jnp
from jax import lax
from jax.experimental import pallas as pl
from jax.experimental.pallas import tpu as pltpu
from jax.sharding import PartitionSpec as P


D = 2048
NOPE = 64
ROPE = 32
HALF = 128
BLOCK = 256
HEADS = 12
LOCAL_HEADS = 6
PLANE = 16
ROWS = 304
CAPACITY = 8
EXPERTS = 64
CHUNKS = 1
PIECES = 4
AHEAD = 3
DEPTH = CAPACITY // CHUNKS
PART = EXPERTS * DEPTH
SPAN = NOPE + ROPE
QW = LOCAL_HEADS * SPAN
PACK = QW + 4 * BLOCK
STATS = HEADS * NOPE
ROWS_OUT = STATS + 32
epsilon = 1e-06
ATTEND_MIB = 24
LOW = -1e30
SCALE = (NOPE + ROPE) ** -0.5 * math.log2(math.e)
f32 = jnp.float32
bf16 = jnp.bfloat16


def vmem():
    return pl.BlockSpec(memory_space=pltpu.VMEM)


def smem():
    return pl.BlockSpec(memory_space=pltpu.SMEM)


def hbm():
    return pl.BlockSpec(memory_space=pltpu.HBM)


def far(x):
    return pltpu.with_memory_space_constraint(x, pltpu.HBM)


def params(mib):
    return pltpu.CompilerParams(vmem_limit_bytes=mib * 1024 * 1024)


def lanes(rows):
    return lax.broadcasted_iota(jnp.int32, (rows, 128), 1)


def turn(first, second, cosine, sine):
    return first * cosine - second * sine, second * cosine + first * sine


def prep_kernel(*refs):
    inputs, (pay_ref, pack_ref) = refs[:8], refs[8:10]
    held, sems = refs[10:18], refs[18]
    copies = [pltpu.make_async_copy(src, dst, sems.at[i]) for i, (src, dst) in enumerate(zip(inputs, held))]
    for copy in copies:
        copy.start()
    for copy in copies:
        copy.wait()
    q_ref, lat_ref, rope_ref, doc_ref, wk_ref, wv_ref, cos_ref, sin_ref = held
    half = lax.axis_index("tp")
    cosine, sine = cos_ref[...], sin_ref[...]
    mine = pl.ds(pl.multiple_of(half * HALF, HALF), HALF)
    pay_ref[0:128, :] = lat_ref[mine, 0:128]
    pay_ref[128:256, :] = lat_ref[mine, 128:256]
    rope = rope_ref[...].astype(f32)
    turned = jnp.concatenate(turn(rope[:16], rope[16:], cosine, sine), axis=0)
    turned = jnp.where(half == 0, turned[:, :128], turned[:, 128:])
    turned = jnp.concatenate([turned, jnp.zeros((96, 128), f32)], axis=0).T
    packed = turned[0:32, :]
    for c in range(1, 4):
        packed = packed + pltpu.roll(turned[32 * c : 32 * c + 32, :], 32 * c, 1)
    pay_ref[256:288, :] = packed.astype(bf16)
    docs = doc_ref[pl.ds(half, 1), :].astype(f32)
    pay_ref[288:304, :] = jnp.broadcast_to(docs, (16, 128)).astype(bf16)
    lane = lanes(BLOCK)
    for head in range(LOCAL_HEADS):
        start = head * SPAN
        pack_ref[start : start + NOPE, :] = q_ref[start : start + NOPE, :]
        rot = q_ref[start + NOPE : start + SPAN, :].astype(f32)
        rot = jnp.concatenate(turn(rot[:16], rot[16:], cosine, sine), axis=0)
        pack_ref[start + NOPE : start + SPAN, :] = rot.astype(bf16)
    w1 = wk_ref[:, 128:256].astype(f32)
    w2 = wk_ref[:, 256:384].astype(f32)
    r1, r2 = pltpu.roll(w1, 64, 1), pltpu.roll(w2, 64, 1)
    first, second = slice(QW, QW + BLOCK), slice(QW + BLOCK, QW + 2 * BLOCK)
    pack_ref[first, 0:128] = wk_ref[:, 0:128]
    pack_ref[first, 128:256] = jnp.where(lane < 64, w1, 0.0).astype(bf16)
    pack_ref[second, 0:128] = jnp.where(lane < 64, r1, r2).astype(bf16)
    pack_ref[second, 128:256] = jnp.where(lane < 64, r2, 0.0).astype(bf16)
    pack_ref[QW + 2 * BLOCK : QW + 3 * BLOCK, :] = wv_ref[:, 0:256]
    pack_ref[QW + 3 * BLOCK : PACK, 0:128] = wv_ref[:, 256:384]
    pack_ref[QW + 3 * BLOCK : PACK, 128:256] = jnp.zeros((BLOCK, 128), bf16)


def spread_kernel(own_ref, oth_ref, q_ref, v_ref):
    for side, src in enumerate((own_ref, oth_ref)):
        for local in range(LOCAL_HEADS):
            head, at, start = side * LOCAL_HEADS + local, local % 3 * NOPE, local * SPAN
            q_ref[head] = jnp.zeros((256, BLOCK), bf16)
            q_ref[head, at : at + NOPE, :] = src[start : start + NOPE, :]
            q_ref[head, 192 : 192 + ROPE, :] = src[start + NOPE : start + SPAN, :]
        base = QW + 2 * BLOCK
        for panel in range(3):
            rows, cols = base + panel // 2 * BLOCK, panel % 2 * 128
            piece = src[rows : rows + BLOCK, cols : cols + 128].astype(f32).T
            v_ref[side * 384 + panel * 128 : side * 384 + panel * 128 + 128, :] = piece.astype(bf16)


def attend_kernel(late, *refs):
    if late:
        ext_ref, refs = refs[0], refs[1:]
    src_ref, wv_src, q_ref, own_ref, oth_ref, qdoc_ref, doc_ref, mine_ref, theirs_ref = refs[:9]
    k_s, v_s, m_s, l_s, a_s, bias_s, arr_ref, wv_ref, sems = refs[9:]
    fetch = pltpu.make_async_copy(src_ref, arr_ref, sems.at[0])
    fetch.start()
    fetch_wv = pltpu.make_async_copy(wv_src, wv_ref, sems.at[1])
    fetch_wv.start()
    half = lax.axis_index("tp")
    seat = lax.axis_index("sp")
    plane, spot = seat // PLANE, seat % PLANE
    doc_first = doc_ref[0].astype(f32)
    doc_last = doc_ref[BLOCK - 1].astype(f32)
    m_s[...] = jnp.full(m_s.shape, LOW, f32)
    l_s[...] = jnp.zeros(l_s.shape, f32)
    a_s[...] = jnp.zeros(a_s.shape, f32)
    fetch.wait()
    fetch_wv.wait()

    def block_of(i):
        if not late:
            return (plane - 1) * PLANE + i
        return (plane - jnp.where(i <= spot, 0, 2)) * PLANE + i

    def place(block):
        return jnp.where(block >= 0, block * BLOCK + half * HALF, -1)

    groups = [[(arr_ref, 8 * t + b, block_of(8 * t + b)) for b in range(8)] for t in range(2)]
    if late:
        groups.append([(ext_ref, None, (plane - 2) * PLANE + spot)])
    row_lane = lax.broadcasted_iota(jnp.int32, (1, 128), 1)
    code = jnp.zeros((1, 128), f32)
    for t, group in enumerate(groups):
        high = low = None
        for ref, i, block in group:
            docs = (ref[288:304, :] if i is None else ref[i, 288:304, :]).astype(f32)[0:1, :]
            seen = jnp.where(block >= 0, docs, -1.0)
            bound = jnp.where(block == seat, -1.0, seen)
            high = seen if high is None else jnp.maximum(high, seen)
            low = bound if low is None else jnp.minimum(low, bound)
        code = code + jnp.where((row_lane == 127) & (high >= doc_first), float(2 ** (2 * t)), 0.0)
        code = code + jnp.where((row_lane == 0) & (low == doc_last), float(2 ** (2 * t + 1)), 0.0)
    code = jnp.sum(code).astype(jnp.int32)

    def heads(count, masked):
        def side(number, carried):
            first = number * LOCAL_HEADS

            def score(head):
                return jnp.dot(k_s[2 * number + head // 3, :count, :], q_ref[first + head], preferred_element_type=f32)

            following = score(0)
            for head in range(LOCAL_HEADS):
                s = following
                if head + 1 < LOCAL_HEADS:
                    following = score(head + 1)
                at = first + head
                if masked:
                    s = s + bias_s[:count, :]
                old = m_s[at]
                new = jnp.maximum(old, jnp.max(s, axis=0, keepdims=True))
                keep = jnp.exp2((old - new) * SCALE)
                m_s[at] = new
                weights = jnp.exp2((s - new) * SCALE)
                l_s[at] = l_s[at] * keep + jnp.sum(weights, axis=0, keepdims=True)
                rows = pl.ds(pl.multiple_of(at * NOPE, NOPE), NOPE)
                a_s[at] = a_s[at] * keep + jnp.dot(v_s[rows, :count], weights.astype(bf16), preferred_element_type=f32)
            return carried

        lax.fori_loop(0, 2, side, 0)

    def tile(load, blocks, flags):
        panels = len(blocks)
        count = panels * 128
        active = (flags & 1) == 1
        plain = (flags & 2) == 2

        @pl.when(active)
        def _():
            lat = jnp.concatenate(
                [
                    jnp.concatenate([load(b, 0, 128) for b in range(panels)], axis=0),
                    jnp.concatenate([load(b, 128, 256) for b in range(panels)], axis=0),
                ],
                axis=1,
            )
            turned = []
            for b in range(panels):
                r = load(b, 256, 288).astype(f32)
                turned += [pltpu.roll(r, 64, 1), pltpu.roll(r, 32, 1), r, pltpu.roll(r, 96, 1)]
            turned = jnp.concatenate(turned, axis=0)
            wide = lanes(count)
            turned = jnp.where((wide >= 64) & (wide < 96), turned, 0.0)
            for side, src in enumerate((own_ref, oth_ref)):
                for g in range(2):
                    rows = QW + g * BLOCK
                    keys = jnp.dot(lat, src[rows : rows + BLOCK, :], preferred_element_type=f32)
                    k_s[side * 2 + g, :count, 0:128] = keys[:, 0:128].astype(bf16)
                    k_s[side * 2 + g, :count, 128:256] = (keys[:, 128:256] + turned).astype(bf16)
            v_s[:, :count] = lax.dot_general(
                wv_ref[...], lat, (((1,), (1,)), ((), ())), preferred_element_type=f32
            ).astype(bf16)

        if panels > 1:

            @pl.when(active & plain)
            def _():
                heads(count, False)

        @pl.when(active & jnp.logical_not(plain) if panels > 1 else active)
        def _():
            at_query = seat * BLOCK + lax.broadcasted_iota(jnp.int32, (128, BLOCK), 1)
            row = lax.broadcasted_iota(jnp.int32, (128, BLOCK), 0)
            for b in range(panels):
                base = place(blocks[b])
                at_key = jnp.where(base >= 0, base, 1 << 20) + row
                docs = jnp.broadcast_to(load(b, 288, 304).astype(f32)[0:1, :], (128, 128)).T
                same = jnp.concatenate([docs, docs], axis=1) == qdoc_ref[...]
                bias_s[128 * b : 128 * b + 128, :] = jnp.where((at_key <= at_query) & same, 0.0, LOW)
            heads(count, True)

    if late:
        tile(lambda b, lo, hi: ext_ref[lo:hi, :], [groups[2][0][2]], code >> 4)

    def step(number, carried):
        blocks = [block_of(number * 8 + b) for b in range(8)]
        tile(lambda b, lo, hi: arr_ref[number * 8 + b, lo:hi, :], blocks, code >> (2 * number))
        return carried

    lax.fori_loop(0, 2, step, 0)

    def sides(x):
        left, right = x[:, 0:128], x[:, 128:256]
        return jnp.where(half == 0, left, right), jnp.where(half == 0, right, left)

    for head in range(HEADS):
        at = head + jnp.where(half == 0, 0, LOCAL_HEADS if head < LOCAL_HEADS else -LOCAL_HEADS)
        rows = pl.ds(pl.multiple_of(at * NOPE, NOPE), NOPE)
        mine_ref[rows, :], theirs_ref[rows, :] = sides(a_s[head])
        for base, ref in ((STATS, m_s), (STATS + 16, l_s)):
            mine_ref[pl.ds(base + at, 1), :], theirs_ref[pl.ds(base + at, 1), :] = sides(ref[head])


def slots_of(ids):
    expert = lax.broadcasted_iota(jnp.int32, (EXPERTS, HALF), 0)
    named = [(ids[k : k + 1, :] == expert) for k in range(2)]
    counts = named[0].astype(f32) + named[1].astype(f32)
    row = lax.broadcasted_iota(jnp.int32, (HALF, HALF), 0)
    col = lax.broadcasted_iota(jnp.int32, (HALF, HALF), 1)
    earlier = jnp.dot(counts.astype(bf16), (row < col).astype(f32).astype(bf16), preferred_element_type=f32)
    slot = lax.broadcasted_iota(jnp.int32, (PART, HALF), 0)
    picks = []
    for k in range(2):
        rank = jnp.sum(jnp.where(named[k], earlier, 0.0), axis=0, keepdims=True).astype(jnp.int32)
        base = ids[k : k + 1, :] * DEPTH + rank
        chunks = []
        for c in range(CHUNKS):
            here = (rank >= DEPTH * c) & (rank < DEPTH * (c + 1))
            at = jnp.where(here, base - DEPTH * c, -1)
            chunks.append((slot == at).astype(f32).astype(bf16))
        picks.append(chunks)
    return picks


def norm_of(x):
    return lax.rsqrt(jnp.mean(x * x, axis=-1, keepdims=True) + epsilon)


def mix_kernel(*refs):
    parts, (proj_ref, res_ref, mixg_ref, moeg_ref, ids_ref, mid_ref), rest = refs[:4], refs[4:10], refs[10:]
    buf_refs, held, sems = rest[:CHUNKS], rest[CHUNKS], rest[CHUNKS + 1]
    tops = [part[STATS : STATS + HEADS, :] for part in parts]
    top = jnp.maximum(jnp.maximum(tops[0], tops[1]), jnp.maximum(tops[2], tops[3]))
    shares = [jnp.exp2((s - top) * SCALE) for s in tops]
    total = 0.0
    for part, share in zip(parts, shares):
        total = total + share * part[STATS + 16 : STATS + 16 + HEADS, :]
    pieces = []
    for head in range(HEADS):
        rows = slice(head * NOPE, head * NOPE + NOPE)
        value = 0.0
        for part, share in zip(parts, shares):
            value = value + part[rows, :] * share[head : head + 1, :]
        pieces.append((value / total[head : head + 1, :]).astype(bf16))
    attended = jnp.concatenate(pieces, axis=0)
    mix = lax.dot_general(attended, proj_ref[...], (((0,), (0,)), ((), ())), preferred_element_type=f32)
    branch = mix * norm_of(mix) * mixg_ref[...]
    middle = (res_ref[...].astype(f32) + branch).astype(bf16)
    mid_ref[...] = middle
    wide = middle.astype(f32)
    normed = (wide * norm_of(wide) * moeg_ref[...]).astype(bf16)
    picks = slots_of(ids_ref[...])
    copies = []
    for c in range(CHUNKS):
        chosen = picks[0][c] + picks[1][c]
        for r in range(PIECES):
            rows = slice(r * PART // PIECES, (r + 1) * PART // PIECES)
            held[c, rows, :] = jnp.dot(chosen[rows], normed, preferred_element_type=f32).astype(bf16)
            copies.append(pltpu.make_async_copy(held.at[c, rows], buf_refs[c].at[rows], sems.at[c * PIECES + r]))
            copies[-1].start()
    for copy in copies:
        copy.wait()


def expert_kernel(rows_ref, *refs):
    weights, out_ref, held, first_s, sems = refs[:6], refs[6], refs[7:13], refs[13], refs[14]
    copies = [pltpu.make_async_copy(src, dst, sems.at[i]) for i, (src, dst) in enumerate(zip(weights, held))]
    for copy in copies[:AHEAD]:
        copy.start()
    rows = rows_ref[...]

    def ready(i):
        copies[i].wait()
        if i + AHEAD < len(copies):
            copies[i + AHEAD].start()
        return held[i][...]

    for side in range(2):
        gated = jnp.dot(rows, ready(3 * side), preferred_element_type=f32)
        upward = jnp.dot(rows, ready(3 * side + 1), preferred_element_type=f32)
        hidden = (gated / (1.0 + jnp.exp(-gated)) * upward).astype(bf16)
        part = jnp.dot(hidden, ready(3 * side + 2), preferred_element_type=f32).astype(bf16)
        if side == 0:
            first_s[...] = part
        else:
            out_ref[...] = (first_s[...].astype(f32) + part.astype(f32)).astype(bf16)


def pick_kernel(*refs):
    back_refs, (mid_ref, ids_ref, weight_ref, out_ref) = refs[:CHUNKS], refs[CHUNKS:]
    picks = slots_of(ids_ref[...])
    total = mid_ref[...].astype(f32)
    for k in range(2):
        rows = 0.0
        for c in range(CHUNKS):
            rows = rows + lax.dot_general(
                picks[k][c], back_refs[c][...], (((0,), (0,)), ((), ())), preferred_element_type=f32
            )
        column = jnp.broadcast_to(weight_ref[k : k + 1, :], (HALF, HALF)).T
        total = total + rows * column[:, 0:1]
    out_ref[...] = total.astype(bf16)


def local(
    residual,
    queries,
    latent,
    rope_key,
    doc_ids,
    latent_to_key,
    latent_to_value,
    out_proj,
    mix_gain,
    moe_gain,
    expert_ids,
    route_weight,
    gate_weight,
    up_weight,
    down_weight,
):
    sp = lax.axis_size("sp")
    seat = lax.axis_index("sp")
    spot = seat % PLANE
    swap = [(0, 1), (1, 0)]
    frequency = 10000.0 ** (-jnp.arange(16, dtype=f32) / 16)
    positions = seat * BLOCK + jnp.arange(BLOCK, dtype=jnp.int32)
    angles = positions.astype(f32)[None, :] * frequency[:, None]
    inputs = (queries.T, latent, rope_key.T, doc_ids.reshape(2, 128), latent_to_key, latent_to_value, jnp.cos(angles), jnp.sin(angles))
    payload, pack = pl.pallas_call(
        prep_kernel,
        out_shape=(jax.ShapeDtypeStruct((ROWS, 128), bf16), jax.ShapeDtypeStruct((PACK, BLOCK), bf16)),
        in_specs=[hbm()] * 8,
        out_specs=(vmem(), vmem()),
        scratch_shapes=[pltpu.VMEM(x.shape, x.dtype) for x in inputs] + [pltpu.SemaphoreType.DMA((8,))],
        compiler_params=params(8),
        name="prep",
    )(*map(far, inputs))
    before = []
    for k in (1, 2):
        before.append(lax.ppermute(payload, "sp", [(i, i + PLANE * k) for i in range(sp - PLANE * k)]))
    other = lax.ppermute(pack, "tp", swap)
    target = jnp.arange(PLANE, dtype=jnp.int32)[:, None, None]
    groups = [[z * PLANE + i for i in range(PLANE)] for z in range(sp // PLANE)]

    def plane(x):
        return lax.all_to_all(x, "sp", 0, 0, axis_index_groups=groups, tiled=True)

    late = plane(jnp.where(spot <= target, payload[None], before[1][None]))
    fanned = jnp.broadcast_to(before[0][None], (PLANE, ROWS, 128))
    early = plane(fanned)
    query_docs = doc_ids.astype(f32)[None, :]
    spread = pl.pallas_call(
        spread_kernel,
        out_shape=(jax.ShapeDtypeStruct((HEADS, 256, BLOCK), bf16), pltpu.HBM((STATS, 256), bf16)),
        in_specs=[vmem()] * 2,
        out_specs=(vmem(), vmem()),
        compiler_params=params(6),
        name="spread",
    )(pack, other)
    stat = jax.ShapeDtypeStruct((ROWS_OUT, HALF), f32)

    def attend(is_late, *operands):
        mine, theirs = pl.pallas_call(
            functools.partial(attend_kernel, is_late),
            out_shape=(pltpu.HBM((ROWS_OUT, HALF), f32),) * 2 if is_late else (stat, stat),
            in_specs=[vmem()] * (len(operands) - 1) + [hbm()] * 2 + [vmem()] * 4 + [smem()],
            out_specs=(vmem(), vmem()),
            scratch_shapes=[
                pltpu.VMEM((4, 1024, 256), bf16),
                pltpu.VMEM((STATS, 1024), bf16),
                pltpu.VMEM((HEADS, 1, BLOCK), f32),
                pltpu.VMEM((HEADS, 1, BLOCK), f32),
                pltpu.VMEM((HEADS, NOPE, BLOCK), f32),
                pltpu.VMEM((1024, BLOCK), f32),
                pltpu.VMEM((PLANE, ROWS, 128), bf16),
                pltpu.VMEM((STATS, 256), bf16),
                pltpu.SemaphoreType.DMA((2,)),
            ],
            compiler_params=pltpu.CompilerParams(vmem_limit_bytes=ATTEND_MIB * 1024 * 1024),
            name="attend_late" if is_late else "attend_early",
        )(*operands[:-1], far(operands[-1]), far(spread[1]), spread[0], pack, other, query_docs, doc_ids)
        return mine, lax.ppermute(theirs, "tp", swap)

    parts = attend(True, before[1], late) + attend(False, early)
    middle, *buffers = pl.pallas_call(
        mix_kernel,
        out_shape=(jax.ShapeDtypeStruct((HALF, D), bf16),) + (pltpu.HBM((PART, D), bf16),) * CHUNKS,
        in_specs=[vmem()] * 9,
        out_specs=(vmem(),) + (hbm(),) * CHUNKS,
        scratch_shapes=[pltpu.VMEM((CHUNKS, PART, D), bf16), pltpu.SemaphoreType.DMA((CHUNKS * PIECES,))],
        compiler_params=params(16),
        name="mix",
    )(*parts, out_proj, residual, mix_gain[None], moe_gain[None], expert_ids.T)
    own = (gate_weight[0], up_weight[0], down_weight[0])
    swapped = tuple(lax.ppermute(w, "tp", swap) for w in own)

    def cross(x):
        return lax.all_to_all(x.reshape(EXPERTS, DEPTH, D), "sp", 0, 0, tiled=True).reshape(PART, D)

    rows = [cross(buffers[c]) for c in range(CHUNKS)]
    back = []
    for c in range(CHUNKS):
        result = pl.pallas_call(
            expert_kernel,
            out_shape=pltpu.HBM((PART, D), bf16),
            in_specs=[vmem()] + [hbm()] * 6,
            out_specs=vmem(),
            scratch_shapes=[pltpu.VMEM(w.shape, bf16) for w in own * 2]
            + [pltpu.VMEM((PART, D), bf16), pltpu.SemaphoreType.DMA((6,))],
            compiler_params=params(28),
            name="experts",
        )(rows[c], *map(far, own + swapped))
        back.append(cross(result))
    return pl.pallas_call(
        pick_kernel,
        out_shape=jax.ShapeDtypeStruct((HALF, D), bf16),
        in_specs=[vmem()] * (CHUNKS + 3),
        out_specs=vmem(),
        compiler_params=params(10),
        name="pick",
    )(*back, middle, expert_ids.T, route_weight.T)


def solution(mesh):
    in_specs = (
        P(("sp", "tp"), None),
        P("sp", "tp"),
        P("sp", None),
        P("sp", None),
        P("sp"),
        P(None, "tp"),
        P(None, "tp"),
        P(),
        P(),
        P(),
        P(("sp", "tp"), None),
        P(("sp", "tp"), None),
        P("sp", None, "tp"),
        P("sp", None, "tp"),
        P("sp", "tp", None),
    )
    out_specs = P(("sp", "tp"), None)

    return jax.shard_map(local, mesh=mesh, in_specs=in_specs, out_specs=out_specs, check_vma=False)
```

```python
import functools
import math

import jax
import jax.numpy as jnp
from jax import lax
from jax.experimental import pallas as pl
from jax.experimental.pallas import tpu as pltpu
from jax.sharding import PartitionSpec as P


D = 2048
NOPE = 64
ROPE = 32
HALF = 128
BLOCK = 256
HEADS = 12
LOCAL_HEADS = 6
PLANE = 16
ROWS = 304
CAPACITY = 8
EXPERTS = 64
SLOTS = EXPERTS * CAPACITY
QW = LOCAL_HEADS * 128
KW = 512
VW = 384
PACK = QW + KW + VW
epsilon = 1e-06
ATTEND_MIB = 24
LOW = -1e30
SCALE = (NOPE + ROPE) ** -0.5 * math.log2(math.e)
PIECES = 4
f32 = jnp.float32
bf16 = jnp.bfloat16


def vmem():
    return pl.BlockSpec(memory_space=pltpu.VMEM)


def smem():
    return pl.BlockSpec(memory_space=pltpu.SMEM)


def hbm():
    return pl.BlockSpec(memory_space=pltpu.HBM)


def far(x):
    return pltpu.with_memory_space_constraint(x, pltpu.HBM)


def params(mib):
    return pltpu.CompilerParams(vmem_limit_bytes=mib * 1024 * 1024)


def lanes(rows):
    return lax.broadcasted_iota(jnp.int32, (rows, 128), 1)


def turn(first, second, cosine, sine):
    return first * cosine - second * sine, second * cosine + first * sine


def prep_kernel(*refs):
    inputs, (pay_ref, pack_ref) = refs[:8], refs[8:10]
    held, sems = refs[10:18], refs[18]
    copies = [pltpu.make_async_copy(src, dst, sems.at[i]) for i, (src, dst) in enumerate(zip(inputs, held))]
    for copy in copies:
        copy.start()
    for copy in copies:
        copy.wait()
    q_ref, lat_ref, rope_ref, doc_ref, wk_ref, wv_ref, cos_ref, sin_ref = held
    half = lax.axis_index("tp")
    cosine, sine = cos_ref[...], sin_ref[...]
    mine = pl.ds(pl.multiple_of(half * HALF, HALF), HALF)
    pay_ref[0:128, :] = lat_ref[mine, 0:128]
    pay_ref[128:256, :] = lat_ref[mine, 128:256]
    rope = rope_ref[...].astype(f32)
    turned = jnp.concatenate(turn(rope[:16], rope[16:], cosine, sine), axis=0)
    turned = jnp.where(half == 0, turned[:, :128], turned[:, 128:])
    turned = jnp.concatenate([turned, jnp.zeros((96, 128), f32)], axis=0).T
    packed = turned[0:32, :]
    for c in range(1, 4):
        packed = packed + pltpu.roll(turned[32 * c : 32 * c + 32, :], 32 * c, 1)
    pay_ref[256:288, :] = packed.astype(bf16)
    docs = doc_ref[pl.ds(half, 1), :].astype(f32)
    pay_ref[288:304, :] = jnp.broadcast_to(docs, (16, 128)).astype(bf16)
    lane = lanes(BLOCK)
    for head in range(LOCAL_HEADS):
        start = head * (NOPE + ROPE)
        plain = q_ref[start : start + NOPE, :].astype(f32)
        rot = q_ref[start + NOPE : start + NOPE + ROPE, :].astype(f32)
        x = jnp.concatenate([plain, *turn(rot[:16], rot[16:], cosine, sine), jnp.zeros((32, BLOCK), f32)], axis=0)
        pack_ref[:, head * 128 : head * 128 + 128] = x.T.astype(bf16)
    w0 = wk_ref[:, 0:128]
    w1 = wk_ref[:, 128:256].astype(f32)
    w2 = wk_ref[:, 256:384].astype(f32)
    r1, r2 = pltpu.roll(w1, 64, 1), pltpu.roll(w2, 64, 1)
    pack_ref[:, QW : QW + 128] = w0
    pack_ref[:, QW + 128 : QW + 256] = jnp.where(lane < 64, w1, 0.0).astype(bf16)
    pack_ref[:, QW + 256 : QW + 384] = jnp.where(lane < 64, r1, r2).astype(bf16)
    pack_ref[:, QW + 384 : QW + 512] = jnp.where(lane < 64, r2, 0.0).astype(bf16)
    pack_ref[:, QW + KW : PACK] = wv_ref[...]


def spread_kernel(own_ref, oth_ref, q_ref):
    lane = lanes(BLOCK)
    for head in range(HEADS):
        src = own_ref if head < LOCAL_HEADS else oth_ref
        local = head % LOCAL_HEADS
        x = src[:, local * 128 : local * 128 + 128].astype(f32)
        if head % 3 == 2:
            lo, hi = jnp.zeros_like(x), x
        else:
            lo, hi = jnp.where(lane < 64, x, 0.0), jnp.where(lane < 64, 0.0, x)
            if head % 3 == 1:
                lo = pltpu.roll(lo, 64, 1)
        q_ref[head, :, 0:128] = lo.astype(bf16)
        q_ref[head, :, 128:256] = hi.astype(bf16)


def attend_kernel(late, *refs):
    if late:
        ext_ref, refs = refs[0], refs[1:]
    src_ref, q_ref, own_ref, oth_ref, qdoc_ref, doc_ref, mine_ref, theirs_ref = refs[:8]
    k_s, v_s, m_s, a_s, bias_s, full_s, arr_ref, sem = refs[8:]
    fetch = pltpu.make_async_copy(src_ref, arr_ref, sem)
    fetch.start()
    half = lax.axis_index("tp")
    seat = lax.axis_index("sp")
    plane, spot = seat // PLANE, seat % PLANE
    doc_first = doc_ref[0].astype(f32)
    doc_last = doc_ref[BLOCK - 1].astype(f32)
    lane = lanes(BLOCK)
    m_s[...] = jnp.full(m_s.shape, LOW, f32)
    a_s[...] = jnp.zeros(a_s.shape, f32)
    fetch.wait()

    def block_of(i):
        if not late:
            return (plane - 1) * PLANE + i
        return (plane - jnp.where(i <= spot, 0, 2)) * PLANE + i

    def place(block):
        return jnp.where(block >= 0, block * BLOCK + half * HALF, -1)

    groups = [[(arr_ref, 8 * t + b, block_of(8 * t + b)) for b in range(8)] for t in range(2)]
    if late:
        groups.append([(ext_ref, None, (plane - 2) * PLANE + spot)])
    row_lane = lax.broadcasted_iota(jnp.int32, (1, 128), 1)
    code = jnp.zeros((1, 128), f32)
    for t, group in enumerate(groups):
        high = low = None
        for ref, i, block in group:
            docs = (ref[288:304, :] if i is None else ref[i, 288:304, :]).astype(f32)[0:1, :]
            seen = jnp.where(block >= 0, docs, -1.0)
            bound = jnp.where(block == seat, -1.0, seen)
            high = seen if high is None else jnp.maximum(high, seen)
            low = bound if low is None else jnp.minimum(low, bound)
        code = code + jnp.where((row_lane == 127) & (high >= doc_first), float(2 ** (2 * t)), 0.0)
        code = code + jnp.where((row_lane == 0) & (low == doc_last), float(2 ** (2 * t + 1)), 0.0)
    code = jnp.sum(code).astype(jnp.int32)

    def heads(count, masked):
        panels = count // 128

        def side(number, carried):
            first = number * LOCAL_HEADS

            def score(head):
                return lax.dot_general(
                    q_ref[first + head],
                    k_s[2 * number + head // 3, :count, :],
                    (((1,), (1,)), ((), ())),
                    preferred_element_type=f32,
                )

            following = score(0)
            for head in range(LOCAL_HEADS):
                s = following
                if head + 1 < LOCAL_HEADS:
                    following = score(head + 1)
                at = first + head
                parts = [s[:, 128 * b : 128 * b + 128] for b in range(panels)]
                if masked:
                    parts = [part + bias_s[:, 128 * b : 128 * b + 128] for b, part in enumerate(parts)]
                top = parts[0]
                for part in parts[1:]:
                    top = jnp.maximum(top, part)
                old = m_s[at]
                new = jnp.maximum(old, jnp.max(top, axis=1, keepdims=True))
                keep = jnp.exp2((old - new) * SCALE)
                m_s[at] = new
                weights = [jnp.exp2((part - new) * SCALE).astype(bf16) for part in parts]
                rounded = jnp.concatenate(weights, axis=1) if panels > 1 else weights[0]
                a_s[at] = a_s[at] * keep + jnp.dot(rounded, v_s[at, :count, :], preferred_element_type=f32)
            return carried

        lax.fori_loop(0, 2, side, 0)

    def tile(load, blocks, flags):
        panels = len(blocks)
        count = panels * 128
        active = (flags & 1) == 1
        plain = (flags & 2) == 2

        @pl.when(active)
        def _():
            lat = jnp.concatenate(
                [
                    jnp.concatenate([load(b, 0, 128) for b in range(panels)], axis=0),
                    jnp.concatenate([load(b, 128, 256) for b in range(panels)], axis=0),
                ],
                axis=1,
            )
            turned = []
            for b in range(panels):
                r = load(b, 256, 288).astype(f32)
                turned += [pltpu.roll(r, 64, 1), pltpu.roll(r, 32, 1), r, pltpu.roll(r, 96, 1)]
            turned = jnp.concatenate(turned, axis=0)
            wide = lanes(count)
            turned = jnp.where((wide >= 64) & (wide < 96), turned, 0.0)
            for side, src in enumerate((own_ref, oth_ref)):
                keys = jnp.dot(lat, src[:, QW : QW + KW], preferred_element_type=f32)
                for g in range(2):
                    at = side * 2 + g
                    k_s[at, :count, 0:128] = keys[:, g * 256 : g * 256 + 128].astype(bf16)
                    k_s[at, :count, 128:256] = (keys[:, g * 256 + 128 : g * 256 + 256] + turned).astype(bf16)
                rows = jnp.dot(lat, src[:, QW + KW : PACK], preferred_element_type=f32)
                for pair in range(3):
                    both = rows[:, pair * 128 : pair * 128 + 128]
                    at = side * LOCAL_HEADS + pair * 2
                    v_s[at, :count, :] = jnp.where(wide < 64, both, 1.0).astype(bf16)
                    v_s[at + 1, :count, :] = jnp.where(wide < 64, 1.0, both).astype(bf16)

        if panels > 1:

            @pl.when(active & plain)
            def _():
                heads(count, False)

        @pl.when(active & jnp.logical_not(plain) if panels > 1 else active)
        def _():
            at_query = seat * BLOCK + lax.broadcasted_iota(jnp.int32, (BLOCK, 128), 0)
            for b in range(panels):
                base = place(blocks[b])
                at_key = jnp.where(base >= 0, base, 1 << 20) + lane
                docs = load(b, 288, 304).astype(f32)[0:1, :]
                allowed = (at_key <= at_query) & (docs == qdoc_ref[...])
                bias_s[:, 128 * b : 128 * b + 128] = jnp.where(allowed, 0.0, LOW)
            heads(count, True)

    if late:
        tile(lambda b, lo, hi: ext_ref[lo:hi, :], [groups[2][0][2]], code >> 4)

    def step(number, carried):
        blocks = [block_of(number * 8 + b) for b in range(8)]
        tile(lambda b, lo, hi: arr_ref[number * 8 + b, lo:hi, :], blocks, code >> (2 * number))
        return carried

    lax.fori_loop(0, 2, step, 0)

    stats = jnp.zeros((BLOCK, 128), f32)
    for head in range(HEADS):
        at = head + jnp.where(half == 0, 0, LOCAL_HEADS if head < LOCAL_HEADS else -LOCAL_HEADS)
        stats = jnp.where(lane == at, m_s[head], stats)
        spare = 64 if head % 2 == 0 else 0
        stats = jnp.where(lane == at + 16, a_s[head, :, spare : spare + 1], stats)
    full_s[:, 768:896] = stats
    for pair in range(6):
        both = jnp.where(lane < 64, a_s[2 * pair], a_s[2 * pair + 1])

        @pl.when(half == 0)
        def _():
            full_s[:, pair * 128 : pair * 128 + 128] = both

        @pl.when(half == 1)
        def _():
            at = (pair + 3) % 6
            full_s[:, at * 128 : at * 128 + 128] = both

    mine_ref[...] = full_s[pl.ds(pl.multiple_of(half * HALF, HALF), HALF), :]
    theirs_ref[...] = full_s[pl.ds(pl.multiple_of((1 - half) * HALF, HALF), HALF), :]


def slots_of(ids):
    expert = lax.broadcasted_iota(jnp.int32, (EXPERTS, HALF), 0)
    named = [(ids[k : k + 1, :] == expert) for k in range(2)]
    counts = named[0].astype(f32) + named[1].astype(f32)
    row = lax.broadcasted_iota(jnp.int32, (HALF, HALF), 0)
    col = lax.broadcasted_iota(jnp.int32, (HALF, HALF), 1)
    earlier = jnp.dot(counts.astype(bf16), (row < col).astype(f32).astype(bf16), preferred_element_type=f32)
    slot = lax.broadcasted_iota(jnp.int32, (SLOTS, HALF), 0)
    picks = []
    for k in range(2):
        rank = jnp.sum(jnp.where(named[k], earlier, 0.0), axis=0, keepdims=True)
        at = ids[k : k + 1, :] * CAPACITY + rank.astype(jnp.int32)
        picks.append((slot == at).astype(f32).astype(bf16))
    return picks


def norm_of(x):
    return lax.rsqrt(jnp.mean(x * x, axis=-1, keepdims=True) + epsilon)


def mix_kernel(*refs):
    parts, (proj_ref, res_ref, mixg_ref, moeg_ref, ids_ref, mid_ref, buf_ref, held, sems) = refs[:4], refs[4:]
    lane = lanes(HALF)
    stats = [part[:, 768:896] for part in parts]
    top = jnp.maximum(jnp.maximum(stats[0], stats[1]), jnp.maximum(stats[2], stats[3]))
    shares = [jnp.exp2((s - top) * SCALE) for s in stats]
    panels = []
    for pair in range(6):
        cols = slice(pair * 128, pair * 128 + 128)
        value, total = 0.0, 0.0
        for part, s, share in zip(parts, stats, shares):
            even, odd = share[:, 2 * pair : 2 * pair + 1], share[:, 2 * pair + 1 : 2 * pair + 2]
            scale = jnp.where(lane < 64, even, odd)
            value = value + part[:, cols] * scale
            total = total + scale * jnp.where(lane < 64, s[:, 16 + 2 * pair : 17 + 2 * pair], s[:, 17 + 2 * pair : 18 + 2 * pair])
        panels.append((value / total).astype(bf16))
    attended = jnp.concatenate(panels, axis=1)
    mix = jnp.dot(attended, proj_ref[...], preferred_element_type=f32)
    branch = mix * norm_of(mix) * mixg_ref[...]
    middle = (res_ref[...].astype(f32) + branch).astype(bf16)
    mid_ref[...] = middle
    wide = middle.astype(f32)
    normed = (wide * norm_of(wide) * moeg_ref[...]).astype(bf16)
    picks = slots_of(ids_ref[...])
    chosen = picks[0] + picks[1]
    copies = []
    for r in range(PIECES):
        rows = slice(r * SLOTS // PIECES, (r + 1) * SLOTS // PIECES)
        held[rows, :] = jnp.dot(chosen[rows], normed, preferred_element_type=f32).astype(bf16)
        copies.append(pltpu.make_async_copy(held.at[rows], buf_ref.at[rows], sems.at[r]))
        copies[r].start()
    for copy in copies:
        copy.wait()


def expert_kernel(rows_ref, *refs):
    weights, out_ref, held, first_s, sems = refs[:6], refs[6], refs[7:13], refs[13], refs[14]
    copies = [pltpu.make_async_copy(src, dst, sems.at[i]) for i, (src, dst) in enumerate(zip(weights, held))]
    for copy in copies:
        copy.start()
    rows = rows_ref[...]
    for side in range(2):
        gate, up, down = held[3 * side : 3 * side + 3]
        copies[3 * side].wait()
        gated = jnp.dot(rows, gate[...], preferred_element_type=f32)
        copies[3 * side + 1].wait()
        upward = jnp.dot(rows, up[...], preferred_element_type=f32)
        hidden = (gated / (1.0 + jnp.exp(-gated)) * upward).astype(bf16)
        copies[3 * side + 2].wait()
        part = jnp.dot(hidden, down[...], preferred_element_type=f32).astype(bf16)
        if side == 0:
            first_s[...] = part
        else:
            out_ref[...] = (first_s[...].astype(f32) + part.astype(f32)).astype(bf16)


def pick_kernel(back_ref, mid_ref, ids_ref, weight_ref, out_ref):
    picks = slots_of(ids_ref[...])
    total = mid_ref[...].astype(f32)
    for k in range(2):
        rows = lax.dot_general(picks[k], back_ref[...], (((0,), (0,)), ((), ())), preferred_element_type=f32)
        column = jnp.broadcast_to(weight_ref[k : k + 1, :], (HALF, HALF)).T
        total = total + rows * column[:, 0:1]
    out_ref[...] = total.astype(bf16)


def local(
    residual,
    queries,
    latent,
    rope_key,
    doc_ids,
    latent_to_key,
    latent_to_value,
    out_proj,
    mix_gain,
    moe_gain,
    expert_ids,
    route_weight,
    gate_weight,
    up_weight,
    down_weight,
):
    sp = lax.axis_size("sp")
    seat = lax.axis_index("sp")
    spot = seat % PLANE
    swap = [(0, 1), (1, 0)]
    frequency = 10000.0 ** (-jnp.arange(16, dtype=f32) / 16)
    positions = seat * BLOCK + jnp.arange(BLOCK, dtype=jnp.int32)
    angles = positions.astype(f32)[None, :] * frequency[:, None]
    inputs = (queries.T, latent, rope_key.T, doc_ids.reshape(2, 128), latent_to_key, latent_to_value, jnp.cos(angles), jnp.sin(angles))
    payload, pack = pl.pallas_call(
        prep_kernel,
        out_shape=(jax.ShapeDtypeStruct((ROWS, 128), bf16), jax.ShapeDtypeStruct((BLOCK, PACK), bf16)),
        in_specs=[hbm()] * 8,
        out_specs=(vmem(), vmem()),
        scratch_shapes=[pltpu.VMEM(x.shape, x.dtype) for x in inputs] + [pltpu.SemaphoreType.DMA((8,))],
        compiler_params=params(8),
        name="prep",
    )(*map(far, inputs))
    before = []
    for k in (1, 2):
        before.append(lax.ppermute(payload, "sp", [(i, i + PLANE * k) for i in range(sp - PLANE * k)]))
    other = lax.ppermute(pack, "tp", swap)
    own = (gate_weight[0], up_weight[0], down_weight[0])
    swapped = tuple(lax.ppermute(w, "tp", swap) for w in own)
    target = jnp.arange(PLANE, dtype=jnp.int32)[:, None, None]
    groups = [[z * PLANE + i for i in range(PLANE)] for z in range(sp // PLANE)]

    def plane(x):
        return lax.all_to_all(x, "sp", 0, 0, axis_index_groups=groups, tiled=True)

    late = plane(jnp.where(spot <= target, payload[None], before[1][None]))
    fanned = jnp.broadcast_to(before[0][None], (PLANE, ROWS, 128))
    early = plane(fanned)
    query_docs = jnp.broadcast_to(doc_ids.astype(f32)[:, None], (BLOCK, 128))
    spread = pl.pallas_call(
        spread_kernel,
        out_shape=jax.ShapeDtypeStruct((HEADS, BLOCK, 256), bf16),
        in_specs=[vmem()] * 2,
        out_specs=vmem(),
        compiler_params=params(6),
        name="spread",
    )(pack, other)
    stat = jax.ShapeDtypeStruct((HALF, 896), f32)

    def attend(is_late, *operands):
        mine, theirs = pl.pallas_call(
            functools.partial(attend_kernel, is_late),
            out_shape=(pltpu.HBM((HALF, 896), f32),) * 2 if is_late else (stat, stat),
            in_specs=[vmem()] * (len(operands) - 1) + [hbm()] + [vmem()] * 4 + [smem()],
            out_specs=(vmem(), vmem()),
            scratch_shapes=[
                pltpu.VMEM((4, 1024, 256), bf16),
                pltpu.VMEM((HEADS, 1024, 128), bf16),
                pltpu.VMEM((HEADS, BLOCK, 128), f32),
                pltpu.VMEM((HEADS, BLOCK, 128), f32),
                pltpu.VMEM((BLOCK, 1024), f32),
                pltpu.VMEM((BLOCK, 896), f32),
                pltpu.VMEM((PLANE, ROWS, 128), bf16),
                pltpu.SemaphoreType.DMA(()),
            ],
            compiler_params=params(ATTEND_MIB),
            name="attend_late" if is_late else "attend_early",
        )(*operands[:-1], far(operands[-1]), spread, pack, other, query_docs, doc_ids)
        return mine, lax.ppermute(theirs, "tp", swap)

    parts = attend(True, before[1], late) + attend(False, early)
    middle, buffer = pl.pallas_call(
        mix_kernel,
        out_shape=(jax.ShapeDtypeStruct((HALF, D), bf16), pltpu.HBM((SLOTS, D), bf16)),
        in_specs=[vmem()] * 9,
        out_specs=(vmem(), hbm()),
        scratch_shapes=[pltpu.VMEM((SLOTS, D), bf16), pltpu.SemaphoreType.DMA((PIECES,))],
        compiler_params=params(16),
        name="mix",
    )(*parts, out_proj, residual, mix_gain[None], moe_gain[None], expert_ids.T)
    rows = lax.all_to_all(buffer.reshape(EXPERTS, CAPACITY, D), "sp", 0, 0, tiled=True).reshape(SLOTS, D)
    result = pl.pallas_call(
        expert_kernel,
        out_shape=jax.ShapeDtypeStruct((SLOTS, D), bf16),
        in_specs=[vmem()] + [hbm()] * 6,
        out_specs=vmem(),
        scratch_shapes=[pltpu.VMEM(w.shape, bf16) for w in own * 2]
        + [pltpu.VMEM((SLOTS, D), bf16), pltpu.SemaphoreType.DMA((6,))],
        compiler_params=params(32),
        name="experts",
    )(rows, *map(far, own + swapped)).reshape(EXPERTS, CAPACITY, D)
    back = lax.all_to_all(result, "sp", 0, 0, tiled=True).reshape(SLOTS, D)
    return pl.pallas_call(
        pick_kernel,
        out_shape=jax.ShapeDtypeStruct((HALF, D), bf16),
        in_specs=[vmem()] * 4,
        out_specs=vmem(),
        compiler_params=params(10),
        name="pick",
    )(back, middle, expert_ids.T, route_weight.T)


def solution(mesh):
    in_specs = (
        P(("sp", "tp"), None),
        P("sp", "tp"),
        P("sp", None),
        P("sp", None),
        P("sp"),
        P(None, "tp"),
        P(None, "tp"),
        P(),
        P(),
        P(),
        P(("sp", "tp"), None),
        P(("sp", "tp"), None),
        P("sp", None, "tp"),
        P("sp", None, "tp"),
        P("sp", "tp", None),
    )
    out_specs = P(("sp", "tp"), None)

    return jax.shard_map(local, mesh=mesh, in_specs=in_specs, out_specs=out_specs, check_vma=False)
```

```python
import functools
import math

import jax
import jax.numpy as jnp
from jax import lax
from jax.experimental import pallas as pl
from jax.experimental.pallas import tpu as pltpu
from jax.sharding import PartitionSpec as P


D = 2048
NOPE = 64
ROPE = 32
HALF = 128
BLOCK = 256
HEADS = 12
LOCAL_HEADS = 6
PLANE = 16
ROWS = 304
CAPACITY = 8
EXPERTS = 64
SLOTS = EXPERTS * CAPACITY
QW = LOCAL_HEADS * 128
KW = 512
VW = 384
PACK = QW + KW + VW
epsilon = 1e-06
ATTEND_MIB = 24
LOW = -1e30
SCALE = (NOPE + ROPE) ** -0.5 * math.log2(math.e)
PIECES = 4
f32 = jnp.float32
bf16 = jnp.bfloat16


def vmem():
    return pl.BlockSpec(memory_space=pltpu.VMEM)


def smem():
    return pl.BlockSpec(memory_space=pltpu.SMEM)


def hbm():
    return pl.BlockSpec(memory_space=pltpu.HBM)


def far(x):
    return pltpu.with_memory_space_constraint(x, pltpu.HBM)


def params(mib):
    return pltpu.CompilerParams(vmem_limit_bytes=mib * 1024 * 1024)


def lanes(rows):
    return lax.broadcasted_iota(jnp.int32, (rows, 128), 1)


def turn(first, second, cosine, sine):
    return first * cosine - second * sine, second * cosine + first * sine


def fetch_all(inputs, held, sems):
    copies = [pltpu.make_async_copy(src, dst, sems.at[i]) for i, (src, dst) in enumerate(zip(inputs, held))]
    for copy in copies:
        copy.start()
    for copy in copies:
        copy.wait()


def prep_kernel(*refs):
    pay_ref, held, sems = refs[5], refs[6:11], refs[11]
    fetch_all(refs[:5], held, sems)
    lat_ref, rope_ref, doc_ref, cos_ref, sin_ref = held
    half = lax.axis_index("tp")
    cosine, sine = cos_ref[...], sin_ref[...]
    mine = pl.ds(pl.multiple_of(half * HALF, HALF), HALF)
    pay_ref[0:128, :] = lat_ref[mine, 0:128]
    pay_ref[128:256, :] = lat_ref[mine, 128:256]
    rope = rope_ref[...].astype(f32)
    turned = jnp.concatenate(turn(rope[:16], rope[16:], cosine, sine), axis=0)
    turned = jnp.where(half == 0, turned[:, :128], turned[:, 128:])
    turned = jnp.concatenate([turned, jnp.zeros((96, 128), f32)], axis=0).T
    packed = turned[0:32, :]
    for c in range(1, 4):
        packed = packed + pltpu.roll(turned[32 * c : 32 * c + 32, :], 32 * c, 1)
    pay_ref[256:288, :] = packed.astype(bf16)
    docs = doc_ref[pl.ds(half, 1), :].astype(f32)
    pay_ref[288:304, :] = jnp.broadcast_to(docs, (16, 128)).astype(bf16)


def pack_kernel(*refs):
    pack_ref, held, sems = refs[5], refs[6:11], refs[11]
    fetch_all(refs[:5], held, sems)
    q_ref, wk_ref, wv_ref, cos_ref, sin_ref = held
    cosine, sine = cos_ref[...], sin_ref[...]
    lane = lanes(BLOCK)
    for head in range(LOCAL_HEADS):
        start = head * (NOPE + ROPE)
        plain = q_ref[start : start + NOPE, :].astype(f32)
        rot = q_ref[start + NOPE : start + NOPE + ROPE, :].astype(f32)
        x = jnp.concatenate([plain, *turn(rot[:16], rot[16:], cosine, sine), jnp.zeros((32, BLOCK), f32)], axis=0)
        pack_ref[:, head * 128 : head * 128 + 128] = x.T.astype(bf16)
    w0 = wk_ref[:, 0:128]
    w1 = wk_ref[:, 128:256].astype(f32)
    w2 = wk_ref[:, 256:384].astype(f32)
    r1, r2 = pltpu.roll(w1, 64, 1), pltpu.roll(w2, 64, 1)
    pack_ref[:, QW : QW + 128] = w0
    pack_ref[:, QW + 128 : QW + 256] = jnp.where(lane < 64, w1, 0.0).astype(bf16)
    pack_ref[:, QW + 256 : QW + 384] = jnp.where(lane < 64, r1, r2).astype(bf16)
    pack_ref[:, QW + 384 : QW + 512] = jnp.where(lane < 64, r2, 0.0).astype(bf16)
    pack_ref[:, QW + KW : PACK] = wv_ref[...]


def spread_kernel(own_ref, oth_ref, q_ref):
    lane = lanes(BLOCK)
    for head in range(HEADS):
        src = own_ref if head < LOCAL_HEADS else oth_ref
        local = head % LOCAL_HEADS
        x = src[:, local * 128 : local * 128 + 128].astype(f32)
        if head % 3 == 2:
            lo, hi = jnp.zeros_like(x), x
        else:
            lo, hi = jnp.where(lane < 64, x, 0.0), jnp.where(lane < 64, 0.0, x)
            if head % 3 == 1:
                lo = pltpu.roll(lo, 64, 1)
        q_ref[head, :, 0:128] = lo.astype(bf16)
        q_ref[head, :, 128:256] = hi.astype(bf16)


def attend_kernel(late, *refs):
    if late:
        ext_ref, refs = refs[0], refs[1:]
    src_ref, q_ref, own_ref, oth_ref, qdoc_ref, doc_ref, mine_ref, theirs_ref = refs[:8]
    k_s, v_s, m_s, a_s, bias_s, full_s, arr_ref, sem = refs[8:]
    fetch = pltpu.make_async_copy(src_ref, arr_ref, sem)
    fetch.start()
    half = lax.axis_index("tp")
    seat = lax.axis_index("sp")
    plane, spot = seat // PLANE, seat % PLANE
    doc_first = doc_ref[0].astype(f32)
    doc_last = doc_ref[BLOCK - 1].astype(f32)
    lane = lanes(BLOCK)
    m_s[...] = jnp.full(m_s.shape, LOW, f32)
    a_s[...] = jnp.zeros(a_s.shape, f32)
    fetch.wait()

    def block_of(i):
        if not late:
            return (plane - 1) * PLANE + i
        return (plane - jnp.where(i <= spot, 0, 2)) * PLANE + i

    def place(block):
        return jnp.where(block >= 0, block * BLOCK + half * HALF, -1)

    wide_tile = 8 if late else 16
    tiles = PLANE // wide_tile
    groups = [
        [(arr_ref, wide_tile * t + b, block_of(wide_tile * t + b)) for b in range(wide_tile)] for t in range(tiles)
    ]
    if late:
        groups.append([(ext_ref, None, (plane - 2) * PLANE + spot)])
    row_lane = lax.broadcasted_iota(jnp.int32, (1, 128), 1)
    code = jnp.zeros((1, 128), f32)
    for t, group in enumerate(groups):
        high = low = None
        for ref, i, block in group:
            docs = (ref[288:304, :] if i is None else ref[i, 288:304, :]).astype(f32)[0:1, :]
            seen = jnp.where(block >= 0, docs, -1.0)
            bound = jnp.where(block == seat, -1.0, seen)
            high = seen if high is None else jnp.maximum(high, seen)
            low = bound if low is None else jnp.minimum(low, bound)
        code = code + jnp.where((row_lane == 127) & (high >= doc_first), float(2 ** (2 * t)), 0.0)
        code = code + jnp.where((row_lane == 0) & (low == doc_last), float(2 ** (2 * t + 1)), 0.0)
    code = jnp.sum(code).astype(jnp.int32)

    def heads(count, masked):
        panels = count // 128
        turns = 3 if masked and not late else LOCAL_HEADS

        def side(number, carried):
            first = number * turns

            def score(head):
                return lax.dot_general(
                    q_ref[first + head],
                    k_s[turns // 3 * number + head // 3, :count, :],
                    (((1,), (1,)), ((), ())),
                    preferred_element_type=f32,
                )

            following = score(0)
            for head in range(turns):
                s = following
                if head + 1 < turns:
                    following = score(head + 1)
                at = first + head
                parts = [s[:, 128 * b : 128 * b + 128] for b in range(panels)]
                if masked:
                    parts = [part + bias_s[:, 128 * b : 128 * b + 128] for b, part in enumerate(parts)]
                top = parts[0]
                for part in parts[1:]:
                    top = jnp.maximum(top, part)
                old = m_s[at]
                new = jnp.maximum(old, jnp.max(top, axis=1, keepdims=True))
                keep = jnp.exp2((old - new) * SCALE)
                m_s[at] = new
                weights = [jnp.exp2((part - new) * SCALE).astype(bf16) for part in parts]
                rounded = jnp.concatenate(weights, axis=1) if panels > 1 else weights[0]
                a_s[at] = a_s[at] * keep + jnp.dot(rounded, v_s[at, :count, :], preferred_element_type=f32)
            return carried

        lax.fori_loop(0, HEADS // turns, side, 0)

    def tile(load, blocks, flags):
        panels = len(blocks)
        count = panels * 128
        active = (flags & 1) == 1
        plain = (flags & 2) == 2

        @pl.when(active)
        def _():
            lat = jnp.concatenate(
                [
                    jnp.concatenate([load(b, 0, 128) for b in range(panels)], axis=0),
                    jnp.concatenate([load(b, 128, 256) for b in range(panels)], axis=0),
                ],
                axis=1,
            )
            turned = []
            for b in range(panels):
                r = load(b, 256, 288).astype(f32)
                turned += [pltpu.roll(r, 64, 1), pltpu.roll(r, 32, 1), r, pltpu.roll(r, 96, 1)]
            turned = jnp.concatenate(turned, axis=0)
            wide = lanes(count)
            turned = jnp.where((wide >= 64) & (wide < 96), turned, 0.0)
            for side, src in enumerate((own_ref, oth_ref)):
                keys = jnp.dot(lat, src[:, QW : QW + KW], preferred_element_type=f32)
                for g in range(2):
                    at = side * 2 + g
                    k_s[at, :count, 0:128] = keys[:, g * 256 : g * 256 + 128].astype(bf16)
                    k_s[at, :count, 128:256] = (keys[:, g * 256 + 128 : g * 256 + 256] + turned).astype(bf16)
                rows = jnp.dot(lat, src[:, QW + KW : PACK], preferred_element_type=f32)
                for pair in range(3):
                    both = rows[:, pair * 128 : pair * 128 + 128]
                    at = side * LOCAL_HEADS + pair * 2
                    v_s[at, :count, :] = jnp.where(wide < 64, both, 1.0).astype(bf16)
                    v_s[at + 1, :count, :] = jnp.where(wide < 64, 1.0, both).astype(bf16)

        if panels > 1:

            @pl.when(active & plain)
            def _():
                heads(count, False)

        @pl.when(active & jnp.logical_not(plain) if panels > 1 else active)
        def _():
            at_query = seat * BLOCK + lax.broadcasted_iota(jnp.int32, (BLOCK, 128), 0)
            for b in range(panels):
                base = place(blocks[b])
                at_key = jnp.where(base >= 0, base, 1 << 20) + lane
                docs = load(b, 288, 304).astype(f32)[0:1, :]
                allowed = (at_key <= at_query) & (docs == qdoc_ref[...])
                bias_s[:, 128 * b : 128 * b + 128] = jnp.where(allowed, 0.0, LOW)
            heads(count, True)

    if late:
        tile(lambda b, lo, hi: ext_ref[lo:hi, :], [groups[2][0][2]], code >> 4)

    def step(number, carried):
        blocks = [block_of(number * wide_tile + b) for b in range(wide_tile)]
        tile(lambda b, lo, hi: arr_ref[number * wide_tile + b, lo:hi, :], blocks, code >> (2 * number))
        return carried

    lax.fori_loop(0, tiles, step, 0)

    stats = jnp.zeros((BLOCK, 128), f32)
    for head in range(HEADS):
        at = head + jnp.where(half == 0, 0, LOCAL_HEADS if head < LOCAL_HEADS else -LOCAL_HEADS)
        stats = jnp.where(lane == at, m_s[head], stats)
        spare = 64 if head % 2 == 0 else 0
        stats = jnp.where(lane == at + 16, a_s[head, :, spare : spare + 1], stats)
    full_s[:, 768:896] = stats
    for pair in range(6):
        both = jnp.where(lane < 64, a_s[2 * pair], a_s[2 * pair + 1])

        @pl.when(half == 0)
        def _():
            full_s[:, pair * 128 : pair * 128 + 128] = both

        @pl.when(half == 1)
        def _():
            at = (pair + 3) % 6
            full_s[:, at * 128 : at * 128 + 128] = both

    mine_ref[...] = full_s[pl.ds(pl.multiple_of(half * HALF, HALF), HALF), :]
    theirs_ref[...] = full_s[pl.ds(pl.multiple_of((1 - half) * HALF, HALF), HALF), :]


def slots_of(ids):
    expert = lax.broadcasted_iota(jnp.int32, (EXPERTS, HALF), 0)
    named = [(ids[k : k + 1, :] == expert) for k in range(2)]
    counts = named[0].astype(f32) + named[1].astype(f32)
    row = lax.broadcasted_iota(jnp.int32, (HALF, HALF), 0)
    col = lax.broadcasted_iota(jnp.int32, (HALF, HALF), 1)
    earlier = jnp.dot(counts.astype(bf16), (row < col).astype(f32).astype(bf16), preferred_element_type=f32)
    slot = lax.broadcasted_iota(jnp.int32, (SLOTS, HALF), 0)
    picks = []
    for k in range(2):
        rank = jnp.sum(jnp.where(named[k], earlier, 0.0), axis=0, keepdims=True)
        at = ids[k : k + 1, :] * CAPACITY + rank.astype(jnp.int32)
        picks.append((slot == at).astype(f32).astype(bf16))
    return picks


def norm_of(x):
    return lax.rsqrt(jnp.mean(x * x, axis=-1, keepdims=True) + epsilon)


def mix_kernel(*refs):
    parts, (proj_ref, res_ref, mixg_ref, moeg_ref, ids_ref, mid_ref, buf_ref, held, sems) = refs[:4], refs[4:]
    lane = lanes(HALF)
    stats = [part[:, 768:896] for part in parts]
    top = jnp.maximum(jnp.maximum(stats[0], stats[1]), jnp.maximum(stats[2], stats[3]))
    shares = [jnp.exp2((s - top) * SCALE) for s in stats]
    panels = []
    for pair in range(6):
        cols = slice(pair * 128, pair * 128 + 128)
        value, total = 0.0, 0.0
        for part, s, share in zip(parts, stats, shares):
            even, odd = share[:, 2 * pair : 2 * pair + 1], share[:, 2 * pair + 1 : 2 * pair + 2]
            scale = jnp.where(lane < 64, even, odd)
            value = value + part[:, cols] * scale
            total = total + scale * jnp.where(lane < 64, s[:, 16 + 2 * pair : 17 + 2 * pair], s[:, 17 + 2 * pair : 18 + 2 * pair])
        panels.append((value / total).astype(bf16))
    attended = jnp.concatenate(panels, axis=1)
    mix = jnp.dot(attended, proj_ref[...], preferred_element_type=f32)
    branch = mix * norm_of(mix) * mixg_ref[...]
    middle = (res_ref[...].astype(f32) + branch).astype(bf16)
    mid_ref[...] = middle
    wide = middle.astype(f32)
    normed = (wide * norm_of(wide) * moeg_ref[...]).astype(bf16)
    picks = slots_of(ids_ref[...])
    chosen = picks[0] + picks[1]
    copies = []
    for r in range(PIECES):
        rows = slice(r * SLOTS // PIECES, (r + 1) * SLOTS // PIECES)
        held[rows, :] = jnp.dot(chosen[rows], normed, preferred_element_type=f32).astype(bf16)
        copies.append(pltpu.make_async_copy(held.at[rows], buf_ref.at[rows], sems.at[r]))
        copies[r].start()
    for copy in copies:
        copy.wait()


def expert_kernel(rows_ref, *refs):
    weights, out_ref, held, first_s, sems = refs[:6], refs[6], refs[7:13], refs[13], refs[14]
    copies = [pltpu.make_async_copy(src, dst, sems.at[i]) for i, (src, dst) in enumerate(zip(weights, held))]
    for copy in copies:
        copy.start()
    rows = rows_ref[...]
    for side in range(2):
        gate, up, down = held[3 * side : 3 * side + 3]
        copies[3 * side].wait()
        gated = jnp.dot(rows, gate[...], preferred_element_type=f32)
        copies[3 * side + 1].wait()
        upward = jnp.dot(rows, up[...], preferred_element_type=f32)
        hidden = (gated / (1.0 + jnp.exp(-gated)) * upward).astype(bf16)
        copies[3 * side + 2].wait()
        part = jnp.dot(hidden, down[...], preferred_element_type=f32).astype(bf16)
        if side == 0:
            first_s[...] = part
        else:
            out_ref[...] = (first_s[...].astype(f32) + part.astype(f32)).astype(bf16)


def pick_kernel(back_ref, mid_ref, ids_ref, weight_ref, out_ref):
    picks = slots_of(ids_ref[...])
    total = mid_ref[...].astype(f32)
    for k in range(2):
        rows = lax.dot_general(picks[k], back_ref[...], (((0,), (0,)), ((), ())), preferred_element_type=f32)
        column = jnp.broadcast_to(weight_ref[k : k + 1, :], (HALF, HALF)).T
        total = total + rows * column[:, 0:1]
    out_ref[...] = total.astype(bf16)


def local(
    residual,
    queries,
    latent,
    rope_key,
    doc_ids,
    latent_to_key,
    latent_to_value,
    out_proj,
    mix_gain,
    moe_gain,
    expert_ids,
    route_weight,
    gate_weight,
    up_weight,
    down_weight,
):
    sp = lax.axis_size("sp")
    seat = lax.axis_index("sp")
    spot = seat % PLANE
    swap = [(0, 1), (1, 0)]
    frequency = 10000.0 ** (-jnp.arange(16, dtype=f32) / 16)
    positions = seat * BLOCK + jnp.arange(BLOCK, dtype=jnp.int32)
    angles = positions.astype(f32)[None, :] * frequency[:, None]
    waves = (jnp.cos(angles), jnp.sin(angles))

    def first(kernel, shape, *inputs):
        inputs = inputs + waves
        return pl.pallas_call(
            kernel,
            out_shape=jax.ShapeDtypeStruct(shape, bf16),
            in_specs=[hbm()] * 5,
            out_specs=vmem(),
            scratch_shapes=[pltpu.VMEM(x.shape, x.dtype) for x in inputs] + [pltpu.SemaphoreType.DMA((5,))],
            compiler_params=params(8),
        )(*map(far, inputs))

    payload = first(prep_kernel, (ROWS, 128), latent, rope_key.T, doc_ids.reshape(2, 128))
    pack = first(pack_kernel, (BLOCK, PACK), queries.T, latent_to_key, latent_to_value)
    before = []
    for k in (1, 2):
        before.append(lax.ppermute(payload, "sp", [(i, i + PLANE * k) for i in range(sp - PLANE * k)]))
    other = lax.ppermute(pack, "tp", swap)
    own = (gate_weight[0], up_weight[0], down_weight[0])
    swapped = tuple(lax.ppermute(w, "tp", swap) for w in own)
    target = jnp.arange(PLANE, dtype=jnp.int32)[:, None, None]
    groups = [[z * PLANE + i for i in range(PLANE)] for z in range(sp // PLANE)]

    def plane(x):
        return lax.all_to_all(x, "sp", 0, 0, axis_index_groups=groups, tiled=True)

    late = plane(jnp.where(spot <= target, payload[None], before[1][None]))
    fanned = jnp.broadcast_to(before[0][None], (PLANE, ROWS, 128))
    early = plane(fanned)
    query_docs = jnp.broadcast_to(doc_ids.astype(f32)[:, None], (BLOCK, 128))
    spread = pl.pallas_call(
        spread_kernel,
        out_shape=jax.ShapeDtypeStruct((HEADS, BLOCK, 256), bf16),
        in_specs=[vmem()] * 2,
        out_specs=vmem(),
        compiler_params=params(6),
        name="spread",
    )(pack, other)
    stat = jax.ShapeDtypeStruct((HALF, 896), f32)

    def attend(is_late, *operands):
        keys = 1024 if is_late else 2048
        mine, theirs = pl.pallas_call(
            functools.partial(attend_kernel, is_late),
            out_shape=(pltpu.HBM((HALF, 896), f32),) * 2 if is_late else (stat, stat),
            in_specs=[vmem()] * (len(operands) - 1) + [hbm()] + [vmem()] * 4 + [smem()],
            out_specs=(vmem(), vmem()),
            scratch_shapes=[
                pltpu.VMEM((4, keys, 256), bf16),
                pltpu.VMEM((HEADS, keys, 128), bf16),
                pltpu.VMEM((HEADS, BLOCK, 128), f32),
                pltpu.VMEM((HEADS, BLOCK, 128), f32),
                pltpu.VMEM((BLOCK, keys), f32),
                pltpu.VMEM((BLOCK, 896), f32),
                pltpu.VMEM((PLANE, ROWS, 128), bf16),
                pltpu.SemaphoreType.DMA(()),
            ],
            compiler_params=params(ATTEND_MIB if is_late else 44),
            name="attend_late" if is_late else "attend_early",
        )(*operands[:-1], far(operands[-1]), spread, pack, other, query_docs, doc_ids)
        return mine, lax.ppermute(theirs, "tp", swap)

    parts = attend(True, before[1], late) + attend(False, early)
    middle, buffer = pl.pallas_call(
        mix_kernel,
        out_shape=(jax.ShapeDtypeStruct((HALF, D), bf16), pltpu.HBM((SLOTS, D), bf16)),
        in_specs=[vmem()] * 9,
        out_specs=(vmem(), hbm()),
        scratch_shapes=[pltpu.VMEM((SLOTS, D), bf16), pltpu.SemaphoreType.DMA((PIECES,))],
        compiler_params=params(16),
        name="mix",
    )(*parts, out_proj, residual, mix_gain[None], moe_gain[None], expert_ids.T)
    rows = lax.all_to_all(buffer.reshape(EXPERTS, CAPACITY, D), "sp", 0, 0, tiled=True).reshape(SLOTS, D)
    result = pl.pallas_call(
        expert_kernel,
        out_shape=jax.ShapeDtypeStruct((SLOTS, D), bf16),
        in_specs=[vmem()] + [hbm()] * 6,
        out_specs=vmem(),
        scratch_shapes=[pltpu.VMEM(w.shape, bf16) for w in own * 2]
        + [pltpu.VMEM((SLOTS, D), bf16), pltpu.SemaphoreType.DMA((6,))],
        compiler_params=params(32),
        name="experts",
    )(rows, *map(far, own + swapped)).reshape(EXPERTS, CAPACITY, D)
    back = lax.all_to_all(result, "sp", 0, 0, tiled=True).reshape(SLOTS, D)
    return pl.pallas_call(
        pick_kernel,
        out_shape=jax.ShapeDtypeStruct((HALF, D), bf16),
        in_specs=[vmem()] * 4,
        out_specs=vmem(),
        compiler_params=params(10),
        name="pick",
    )(back, middle, expert_ids.T, route_weight.T)


def solution(mesh):
    in_specs = (
        P(("sp", "tp"), None),
        P("sp", "tp"),
        P("sp", None),
        P("sp", None),
        P("sp"),
        P(None, "tp"),
        P(None, "tp"),
        P(),
        P(),
        P(),
        P(("sp", "tp"), None),
        P(("sp", "tp"), None),
        P("sp", None, "tp"),
        P("sp", None, "tp"),
        P("sp", "tp", None),
    )
    out_specs = P(("sp", "tp"), None)

    return jax.shard_map(local, mesh=mesh, in_specs=in_specs, out_specs=out_specs, check_vma=False)
```
